256 devices in a mesh: grp: 2 (over y), fs: 16 (over z), tp: 8 (over x, core).
Axes of the slice: x: 4, y: 2, z: 16, core: 2. Of those that a mesh axis runs over, the one named last changes fastest.
The devices are a block of a 4x16x16 slice.
Arguments:
- tokens: bfloat16 [16384, 2048], P(('grp', 'fs'), 'tp'), parts along dimension 0, may hold values from -16 to 16
- attn_gain: float32 [2048], replicated, may hold values from 0.1 to 1.9
- w_query: bfloat16 [2048, 1024], P('fs', 'tp'), may hold values from -0.125 to 0.125
- w_key: bfloat16 [2048, 1024], P('fs', 'tp'), may hold values from -0.125 to 0.125
- w_value: bfloat16 [2048, 2048], P('fs', 'tp'), may hold values from -0.125 to 0.125
- w_low: bfloat16 [2048, 32], replicated, may hold values from -0.125 to 0.125
- w_lift: bfloat16 [32, 1024], P(None, 'tp'), may hold values from -1 to 1
- decay_bias: float32 [1024], P('tp'), may hold values from -0.5 to 6
- head_gain: float32 [256], replicated, may hold values from 0.1 to 1.9
- w_out: bfloat16 [2048, 2048], P('tp', 'fs'), may hold values from -0.125 to 0.125
- ffn_gain: float32 [2048], replicated, may hold values from 0.1 to 1.9
- w_gate: bfloat16 [2048, 5632], P('fs', 'tp'), may hold values from -0.125 to 0.125
- w_up: bfloat16 [2048, 5632], P('fs', 'tp'), may hold values from -0.125 to 0.125
- w_down: bfloat16 [5632, 2048], P('tp', 'fs'), may hold values from -0.078125 to 0.078125
- final_gain: float32 [2048], P('tp'), may hold values from 0.1 to 1.9
Outputs:
- result: bfloat16 [16384, 2048], P(('grp', 'fs'), 'tp'), parts along dimension 0
The draws below stay inside these ranges and needn't reach their ends.
There are 2 independent parts, one for each index of `grp`. The reference program is written for one: setup_inputs(seed, part) draws one part's arguments, and reference() takes and returns one part's arrays. A program takes and returns all parts, laid end to end along the dimension named above; an argument that names none is the same for every part. Nothing has to cross between parts.
All inputs are finite; a program needn't handle non-finite values.
Results may differ from the reference program's by a relative error of at most 0.015.
Values may be sent and summed in bfloat16 or wider, within the bound.
A program may use at most 64 MiB of HBM per device.

```python
import math
import jax
import jax.numpy as jnp
from jax import lax

D = 2048
HEADS = 8
DK = 128
DV = 256
RANK = 32
FF = 5632
BLOCK = 64
LEN = 512
QK = 1024
V = 2048
TOKENS = 8192
N_FS = 16
N_TP = 8


def draw_tokens(key, part):
    first_key, second_key = jax.random.split(jax.random.fold_in(key, 11), 2)
    groups = 8
    scales = jnp.exp(jax.random.uniform(first_key, (groups,), jnp.float32, math.log(0.25), math.log(4.0)))
    scales = jnp.repeat(scales, D // groups)
    base = jnp.clip(jax.random.normal(second_key, (TOKENS, D), jnp.float32), -4.0, 4.0)
    return (base * scales[None, :]).astype(jnp.bfloat16)


def draw_decay_bias(key, part):
    first_key, second_key, third_key = jax.random.split(jax.random.fold_in(key, 23), 3)
    fast_share = 0.5
    is_fast = jax.random.uniform(first_key, (QK,), jnp.float32) < fast_share
    fast_value = jax.random.uniform(second_key, (QK,), jnp.float32, -0.5, 0.5)
    slow_value = jax.random.uniform(third_key, (QK,), jnp.float32, 4.5, 6.0)
    return jnp.where(is_fast, fast_value, slow_value)


def block_levels(stream_key, extent, shards, smallest, high):
    def one(axis_at, shards_of):
        heights = jax.random.uniform(jax.random.fold_in(jax.random.fold_in(stream_key, 6), axis_at), (shards_of,), jnp.float32, smallest / len(shards), high / len(shards))
        return jnp.repeat(jnp.exp(heights), extent[axis_at] // shards_of).reshape((-1,) + (1,) * (len(extent) - axis_at - 1))

    level = one(*shards[0])
    for cut in shards[1:]:
        level = level * one(*cut)
    return level


def noise(key, shape, width, bound, pieces=(), kind=jnp.bfloat16):
    values = width * jax.random.normal(key, shape, jnp.float32)
    if pieces:
        values = values * block_levels(key, shape, pieces, -0.22, 0.18)
    return jnp.clip(values, -bound, bound).astype(kind)


def setup_inputs(seed: int = 0, part: int = 0) -> dict:
    streams_of = jax.random.split(jax.random.key(seed), 16)
    own_keys = jax.random.split(jax.random.fold_in(streams_of[15], part), 16)
    return {
        "tokens": draw_tokens(jax.random.fold_in(jax.random.fold_in(streams_of[15], part), 71), part),
        "attn_gain": jnp.clip(1.0 + 0.18 * jax.random.normal(streams_of[1], (D,), jnp.float32), 0.1, 1.9),
        "w_query": noise(streams_of[2], (D, QK), D ** -0.5, 0.125, ((0, 16), (1, 8))),
        "w_key": noise(streams_of[3], (D, QK), D ** -0.5, 0.125, ((0, 16), (1, 8))),
        "w_value": noise(streams_of[4], (D, V), D ** -0.5, 0.125, ((0, 16), (1, 8))),
        "w_low": noise(streams_of[5], (D, RANK), D ** -0.5, 0.125),
        "w_lift": noise(streams_of[6], (RANK, QK), RANK ** -0.5, 1.0, ((1, 8),)),
        "decay_bias": draw_decay_bias(jax.random.fold_in(streams_of[15], 71), part),
        "head_gain": jnp.clip(1.0 + 0.18 * jax.random.normal(streams_of[8], (DV,), jnp.float32), 0.1, 1.9),
        "w_out": noise(streams_of[9], (V, D), V ** -0.5, 0.125, ((0, 8), (1, 16))),
        "ffn_gain": jnp.clip(1.0 + 0.18 * jax.random.normal(streams_of[10], (D,), jnp.float32), 0.1, 1.9),
        "w_gate": noise(streams_of[11], (D, FF), D ** -0.5, 0.125, ((0, 16), (1, 8))),
        "w_up": noise(streams_of[12], (D, FF), D ** -0.5, 0.125, ((0, 16), (1, 8))),
        "w_down": noise(streams_of[13], (FF, D), FF ** -0.5, 0.078125, ((0, 8), (1, 16))),
        "final_gain": jnp.clip(1.0 + 0.18 * jax.random.normal(streams_of[14], (D,), jnp.float32), 0.1, 1.9),
    }


epsilon = 1e-06
highest = lax.Precision.HIGHEST

def rms_rows(values, gain):
    values = values.astype(jnp.float32)
    factor = lax.rsqrt(lax.optimization_barrier(jnp.mean(values * values, axis=-1, keepdims=True)) + epsilon)
    return values * factor * gain.astype(jnp.float32)

def blockwise_gla(query_rows, key_rows, value_rows, log_decay, head_count):
    length = query_rows.shape[0]
    blocks = length // BLOCK

    def split_heads(array, depth):
        return array.astype(jnp.float32).reshape(blocks, BLOCK, head_count, depth).transpose(2, 0, 1, 3)
    query_f = split_heads(query_rows, DK) * DK ** (-0.5)
    key_f = split_heads(key_rows, DK)
    value_f = split_heads(value_rows, DV)
    log_cum = jnp.cumsum(split_heads(log_decay, DK), axis=2)
    log_last = log_cum[:, :, -1:, :]
    query_dec = query_f * jnp.exp(log_cum)
    key_dec = key_f * jnp.exp(-log_cum)
    causal = jnp.tril(jnp.ones((BLOCK, BLOCK), dtype=bool))
    scores = jnp.where(causal, jnp.einsum('hncd,hnsd->hncs', query_dec, key_dec, precision=highest), 0.0)
    inside = jnp.einsum('hncs,hnsv->hncv', scores, value_f, precision=highest)
    contrib = jnp.einsum('hncd,hncv->hndv', key_f * jnp.exp(log_last - log_cum), value_f, precision=highest)
    decay_block = jnp.exp(log_last[:, :, 0, :])

    def advance(carry_state, inputs):
        decay_step, added = inputs
        return (decay_step[..., None] * carry_state + added, carry_state)
    start_state = jnp.zeros((head_count, DK, DV), jnp.float32)
    final_state, earlier = lax.scan(advance, start_state, (jnp.moveaxis(decay_block, 1, 0), jnp.moveaxis(contrib, 1, 0)))
    earlier = jnp.moveaxis(earlier, 0, 1)
    output = inside + jnp.einsum('hncd,hndv->hncv', query_dec, earlier, precision=highest)
    return output.transpose(1, 2, 0, 3).reshape(length, head_count, DV)

def reference(tokens, attn_gain, w_query, w_key, w_value, w_low, w_lift, decay_bias, head_gain, w_out, ffn_gain, w_gate, w_up, w_down, final_gain):
    normed = rms_rows(tokens, attn_gain).astype(jnp.bfloat16)
    query_rows = jnp.dot(normed, w_query, preferred_element_type=jnp.float32).astype(jnp.bfloat16)
    key_rows = jnp.dot(normed, w_key, preferred_element_type=jnp.float32).astype(jnp.bfloat16)
    value_rows = jnp.dot(normed, w_value, preferred_element_type=jnp.float32).astype(jnp.bfloat16)
    low_rank = jnp.dot(normed, w_low, preferred_element_type=jnp.float32).astype(jnp.bfloat16)
    log_decay = jax.nn.log_sigmoid(jnp.dot(low_rank, w_lift, preferred_element_type=jnp.float32) + decay_bias.astype(jnp.float32)) / 16.0
    gla_out = jax.vmap(lambda qq, kk, vv, gg: blockwise_gla(qq, kk, vv, gg, HEADS))(query_rows.reshape(N_FS, LEN, QK), key_rows.reshape(N_FS, LEN, QK), value_rows.reshape(N_FS, LEN, V), log_decay.reshape(N_FS, LEN, QK))
    gla_out = gla_out.reshape(TOKENS, HEADS, DV)
    mixed_heads = rms_rows(gla_out, head_gain).reshape(TOKENS, V).astype(jnp.bfloat16)
    span = V // N_TP
    attn_sum = jnp.zeros((TOKENS, D), jnp.float32)
    for index in range(N_TP):
        partial_prod = jnp.dot(mixed_heads[:, index * span:(index + 1) * span], w_out[index * span:(index + 1) * span], preferred_element_type=jnp.float32).astype(jnp.bfloat16)
        attn_sum = attn_sum + partial_prod.astype(jnp.float32)
    first_sum = (tokens.astype(jnp.float32) + attn_sum).astype(jnp.bfloat16)
    normed_ffn = rms_rows(first_sum, ffn_gain).astype(jnp.bfloat16)
    gate_rows = jnp.dot(normed_ffn, w_gate, preferred_element_type=jnp.float32)
    up_rows = jnp.dot(normed_ffn, w_up, preferred_element_type=jnp.float32)
    hidden = (jax.nn.silu(gate_rows) * up_rows).astype(jnp.bfloat16)
    units = FF // N_TP
    ffn_sum = jnp.zeros((TOKENS, D), jnp.float32)
    for index in range(N_TP):
        partial_prod = jnp.dot(hidden[:, index * units:(index + 1) * units], w_down[index * units:(index + 1) * units], preferred_element_type=jnp.float32).astype(jnp.bfloat16)
        ffn_sum = ffn_sum + partial_prod.astype(jnp.float32)
    second_sum = first_sum.astype(jnp.float32) + ffn_sum
    return rms_rows(second_sum, final_gain).astype(jnp.bfloat16)
```

```python
import functools

import jax
import jax.numpy as jnp
from jax import lax
from jax.experimental import pallas as pl
from jax.experimental.pallas import tpu as pltpu
from jax.sharding import PartitionSpec as P

DK = 128
DV = 256
BLOCK = 64
EPS = 1e-06
BF = jnp.bfloat16
F32 = jnp.float32
MESH = pl.DeviceIdType.MESH
HIGHEST = lax.Precision.HIGHEST


def dot(a, b, dims=((1,), (0,)), precision=None):
    return lax.dot_general(
        a, b, (dims, ((), ())), precision=precision, preferred_element_type=F32
    )


def kernel(
    n_fs, n_tp,
    tok, wq, wk, wv, wo, wg, wu, wt, wd, wl, ag, wlift, bias, hg, fg, fin,
    out,
    X, Gq, Go, Gg, Gd, N, QKV, C, M, F, H, SS, Q, state,
    PB1, D1, S1, B1, A1, PB2, D2, S2, B2, A2,
    lsem, zs, zr, ys, yr, xs, xr,
):
    rows, width = tok.shape
    d_model = width * n_tp
    half_rows = rows // 2
    half = n_fs // 2
    full = wt.shape[1] * 5 if False else (wg.shape[1] // 128) * 128
    units = wg.shape[1]
    kq, ko, kd = wq.shape[0], wo.shape[0], wd.shape[0]

    grp, z, me = lax.axis_index("grp"), lax.axis_index("fs"), lax.axis_index("tp")
    parity = lax.rem(grp, 2)
    partner = {"grp": grp + 1 - 2 * parity}
    z_up, z_down = {"fs": lax.rem(z + 1, n_fs)}, {"fs": lax.rem(z + n_fs - 1, n_fs)}
    core = lax.rem(me, 2)

    def at_tp(offset):
        return lax.rem(me + offset + n_tp, n_tp)

    def other(slot):
        return slot + 1 - 2 * core

    r_slot, l_slot, o_slot = at_tp(2), at_tp(-2), at_tp(4)
    right, left, sib = {"tp": r_slot}, {"tp": l_slot}, {"tp": other(me)}
    sends = []

    def remote(src, dst, ssem, rsem, device):
        return pltpu.make_async_remote_copy(
            src_ref=src, dst_ref=dst, send_sem=ssem, recv_sem=rsem,
            device_id=device, device_id_type=MESH,
        )

    def send(src, dst, ssem, rsem, device):
        copy = remote(src, dst, ssem, rsem, device)
        copy.start()
        sends.append((src, dst, ssem, rsem, device))

    def arrived(ref, ssem, rsem):
        remote(ref, ref, ssem, rsem, sib).wait_recv()

    zq = pl.multiple_of(z * kq, kq)
    local = [
        (tok, X.at[me]),
        (wq, Gq.at[pl.ds(zq, kq), pl.ds(0, DK)]),
        (wk, Gq.at[pl.ds(zq, kq), pl.ds(DK, DK)]),
        (wv, Gq.at[pl.ds(zq, kq), pl.ds(2 * DK, DV)]),
        (wg.at[:, pl.ds(0, full)], Gg.at[pl.ds(zq, kq), pl.ds(0, full)]),
        (wu.at[:, pl.ds(0, full)], Gg.at[pl.ds(zq, kq), pl.ds(full, full)]),
        (wt, Gg.at[pl.ds(zq, kq), pl.ds(2 * full, 128)]),
        (wo, Go.at[z]),
        (wd, Gd.at[z, pl.ds(0, kd), :]),
    ]
    local = [pltpu.make_async_copy(s, d, lsem.at[i]) for i, (s, d) in enumerate(local)]
    for copy in local:
        copy.start()

    barrier = pltpu.get_barrier_semaphore()
    greeted = [z_up, z_down, partner] + [{"tp": at_tp(k)} for k in range(1, n_tp)]
    for device in greeted:
        pl.semaphore_signal(barrier, inc=1, device_id=device, device_id_type=MESH)
    if kd < Gd.shape[1]:
        Gd[:, kd:, :] = jnp.zeros((n_fs, Gd.shape[1] - kd, 128), BF)
        H[:, units:] = jnp.zeros((rows, H.shape[1] - units), BF)
    pl.semaphore_wait(barrier, len(greeted))

    def by_rows(view, base, total, edge):
        chunk, other_edge = total - edge, total - edge

        def part(shard, start, size):
            return view(shard, pl.multiple_of(base + start, 16), size)

        first = (chunk // 2 + 15) // 16 * 16
        return dict(
            ring=lambda s: part(s, parity * edge, chunk),
            mine=lambda s: part(s, parity * other_edge, edge),
            theirs=lambda s: part(s, (1 - parity) * other_edge, edge),
            halves=(
                lambda s: part(s, parity * edge, first),
                lambda s: part(s, parity * edge + first, chunk - first),
            ),
        )

    def gate_up(base, size):
        total = Gg.shape[1]
        edge = (total // 128 * 3 // 8) * 128
        chunk = total - edge

        def part(shard, r0, rn, start, cols):
            row = pl.multiple_of(shard * kq + base + r0, 16)
            return Gg.at[pl.ds(row, rn), pl.ds(pl.multiple_of(start, 128), cols)]

        return dict(
            ring=lambda s: part(s, 0, size, parity * edge, chunk),
            mine=lambda s: part(s, 0, size, parity * chunk, edge),
            theirs=lambda s: part(s, 0, size, (1 - parity) * chunk, edge),
            halves=(
                lambda s: part(s, 0, size // 2, parity * edge, chunk),
                lambda s: part(s, size // 2, size // 2, parity * edge, chunk),
            ),
        )

    def view_q(shard, start, size):
        return Gq.at[pl.ds(pl.multiple_of(shard * kq + start, 16), size), :]

    streams = [
        by_rows(view_q, 0, kq, 48),
        by_rows(lambda s, start, size: Go.at[s, pl.ds(start, size), :], 0, ko, 80),
    ]
    streams += [gate_up(k * 32, 32) for k in range(kq // 32)]
    half_d = kd // 2
    streams += [
        by_rows(lambda s, start, size: Gd.at[s, pl.ds(start, size), :], k * half_d, half_d, 96)
        for k in range(2)
    ]
    QS, OS, G0, G1, G2, G3, E0, E1 = range(8)

    def launch(i):
        ref = streams[i]["ring"](z)
        send(ref, ref, zs.at[i, 0, 0], zr.at[i, 0, 0], z_up)
        send(ref, ref, zs.at[i, 1, 0], zr.at[i, 1, 0], z_down)

    def event(i, s):
        st = streams[i]
        for way, (shard, device) in enumerate(
            ((lax.rem(z - s + n_fs, n_fs), z_up), (lax.rem(z + s, n_fs), z_down))
        ):
            if s < half:
                arrived(st["ring"](shard), zs.at[i, way, s - 1], zr.at[i, way, s - 1])
                ref = st["ring"](shard) if s + 1 < half else st["halves"][way](shard)
                send(ref, ref, zs.at[i, way, s], zr.at[i, way, s], device)
            else:
                ref = st["halves"][way](shard)
                arrived(ref, zs.at[i, way, s - 1], zr.at[i, way, s - 1])
            if s < half or way == 1:
                ref = st["mine"](shard)
                send(ref, ref, ys.at[i, way, s - 1], yr.at[i, way, s - 1], partner)

    def imported(i):
        for s in range(1, half + 1):
            for way, shard in enumerate((lax.rem(z - s + n_fs, n_fs), lax.rem(z + s, n_fs))):
                if s < half or way == 1:
                    ref = streams[i]["theirs"](shard)
                    arrived(ref, ys.at[i, way, s - 1], yr.at[i, way, s - 1])

    queue = []

    def serve(count):
        for _ in range(min(count, len(queue))):
            item = queue.pop(0)
            if item[1] == 0:
                launch(item[0])
            else:
                event(*item)

    top, low = pl.ds(0, half_rows), pl.ds(half_rows, half_rows)

    def gather_stages(buf, base):
        def go(k, slot, part, device):
            ref = buf.at[slot] if part is None else buf.at[slot, part, :]
            send(ref, ref, xs.at[base + k], xr.at[base + k], device)

        def got(k, slot, part):
            ref = buf.at[slot] if part is None else buf.at[slot, part, :]
            arrived(ref, xs.at[base + k], xr.at[base + k])

        def s0():
            go(0, me, top, right)
            go(2, me, low, left)
            go(1, me, low, right)
            go(3, me, top, left)
            go(4, me, None, sib)

        def s1():
            got(0, l_slot, top)
            go(5, l_slot, top, right)
            go(6, l_slot, top, sib)
            got(2, r_slot, low)
            go(7, r_slot, low, left)
            go(8, r_slot, low, sib)

        def s2():
            got(1, l_slot, low)
            go(9, l_slot, low, sib)
            got(3, r_slot, top)
            go(10, r_slot, top, sib)

        def s3():
            got(5, o_slot, top)
            go(11, o_slot, top, sib)
            got(7, o_slot, low)
            go(12, o_slot, low, sib)

        def s4():
            got(4, other(me), None)
            got(6, other(l_slot), top)
            got(8, other(r_slot), low)
            got(9, other(l_slot), low)
            got(10, other(r_slot), top)
            got(11, other(o_slot), top)
            got(12, other(o_slot), low)

        return s0, s1, s2, s3, s4

    def scatter_stages(PB, D, S, B, A, base):
        def go(k, src, dst, device):
            send(src, dst, xs.at[base + k], xr.at[base + k], device)

        def got(k, dst):
            arrived(dst, xs.at[base + k], xr.at[base + k])

        def add(dst, start, count, terms):
            step = 64

            @pl.loop(0, count // step)
            def _(t):
                r = pl.ds(pl.multiple_of(start + t * step, step), step)
                total = terms[0](r).astype(F32)
                for term in terms[1:]:
                    total = total + term(r).astype(F32)
                dst[r, :] = total.astype(BF)

        def s0():
            for k, slot in enumerate((o_slot, r_slot, l_slot, me)):
                go(k, PB.at[other(slot)], D.at[k], sib)

        def s1():
            got(0, D.at[0])
            add(S.at[0], 0, rows, [lambda r: PB[o_slot, r, :], lambda r: D[0, r, :]])
            go(4, S.at[0, top, :], A.at[0], right)
            go(5, S.at[0, low, :], A.at[1], left)
            got(1, D.at[1])
            add(S.at[1], half_rows, half_rows, [lambda r: PB[r_slot, r, :], lambda r: D[1, r, :]])
            go(6, S.at[1, low, :], B.at[0, low, :], right)
            got(2, D.at[2])
            add(S.at[2], 0, half_rows, [lambda r: PB[l_slot, r, :], lambda r: D[2, r, :]])
            go(7, S.at[2, top, :], B.at[1, top, :], left)

        def s2():
            got(4, A.at[0])
            add(S.at[1], 0, half_rows,
                [lambda r: PB[r_slot, r, :], lambda r: D[1, r, :], lambda r: A[0, r, :]])
            go(8, S.at[1, top, :], B.at[0, top, :], right)
            got(5, A.at[1])

            @pl.loop(0, half_rows // 64)
            def _(t):
                ra = pl.ds(pl.multiple_of(t * 64, 64), 64)
                r = pl.ds(pl.multiple_of(half_rows + t * 64, 64), 64)
                total = PB[l_slot, r, :].astype(F32) + D[2, r, :].astype(F32) + A[1, ra, :].astype(F32)
                S[2, r, :] = total.astype(BF)

            go(9, S.at[2, low, :], B.at[1, low, :], left)

        def s3():
            got(3, D.at[3])
            got(6, B.at[0, low, :])
            got(7, B.at[1, top, :])
            got(8, B.at[0, top, :])
            got(9, B.at[1, low, :])

        def own(r):
            return (
                PB[me, r, :].astype(F32) + D[3, r, :].astype(F32)
                + B[0, r, :].astype(F32) + B[1, r, :].astype(F32)
            )

        return s0, s1, s2, s3, own

    def normalize(buf, gain):
        step = 32

        @pl.loop(0, rows // step)
        def _(t):
            r = pl.ds(pl.multiple_of(t * step, step), step)
            blocks = [buf[j, r, :].astype(F32) for j in range(n_tp)]
            squares = blocks[0] * blocks[0]
            for b in blocks[1:]:
                squares = squares + b * b
            factor = lax.rsqrt(jnp.sum(squares, axis=1, keepdims=True) * (1.0 / d_model) + EPS)
            for j, b in enumerate(blocks):
                cols = pl.ds(j * width, width)
                N[r, cols] = (b * factor * gain[:, cols]).astype(BF)

    ti = lax.broadcasted_iota(jnp.int32, (BLOCK, BLOCK), 0)
    si = lax.broadcasted_iota(jnp.int32, (BLOCK, BLOCK), 1)

    def decay():
        tril = jnp.where(ti >= si, 1.0, 0.0).astype(BF)
        step = 2 * BLOCK

        @pl.loop(0, rows // step)
        def _(t):
            r = pl.ds(pl.multiple_of(t * step, step), step)
            rank = dot(N[r, :], wl[...]).astype(BF)
            v = dot(rank, wlift[...]) + bias[...]
            log_decay = (jnp.minimum(v, 0.0) - jnp.log1p(jnp.exp(-jnp.abs(v)))) * (1.0 / 16.0)
            for k in range(2):
                part = log_decay[k * BLOCK : (k + 1) * BLOCK]
                hi = part.astype(BF)
                lo = (part - hi.astype(F32)).astype(BF)
                r2 = pl.ds(pl.multiple_of(t * step + k * BLOCK, BLOCK), BLOCK)
                C[r2, :] = dot(tril, hi) + dot(tril, lo)

    def project(t):
        step = rows // 4
        r = pl.ds(t * step, step)
        QKV[r, :] = dot(N[r, :], Gq[...]).astype(BF)

    def attend(t):
        r = pl.ds(t * BLOCK, BLOCK)
        c = C[r, :]
        last = C[pl.ds((t + 1) * BLOCK - 1, 1), :]
        q = QKV[r, pl.ds(0, DK)].astype(F32) * DK ** (-0.5)
        k = QKV[r, pl.ds(DK, DK)].astype(F32)
        v = QKV[r, pl.ds(2 * DK, DV)]
        q_dec = (q * jnp.exp(c)).astype(BF)
        k_dec = (k * jnp.exp(-c)).astype(BF)
        k_end = (k * jnp.exp(last - c)).astype(BF)
        scores = jnp.where(ti >= si, dot(q_dec, k_dec, ((1,), (1,))), 0.0).astype(BF)
        o = dot(scores, v)
        if t > 0:
            o = o + dot(q_dec, state[...].astype(BF), ((1,), (1,)))
        added = dot(v, k_end, ((0,), (0,)))
        state[...] = state[...] * jnp.exp(last) + added if t > 0 else added
        factor = lax.rsqrt(jnp.mean(o * o, axis=1, keepdims=True) + EPS)
        M[r, :] = (o * factor * hg[...]).astype(BF)

    def partial_products(left_ref, G, PB):
        step = rows // 2

        @pl.loop(0, n_tp)
        def _(j):
            weight = jnp.concatenate([G[2 * j], G[2 * j + 1]], axis=1)
            for t in range(2):
                r = pl.ds(t * step, step)
                PB[j, r, :] = dot(left_ref[r, :], weight).astype(BF)

    def feed(t, at, size):
        step = rows // 2
        r = pl.ds(t * step, step)
        if at < full:
            gate = dot(N[r, :], Gg[:, pl.ds(at, size)])
            up = dot(N[r, :], Gg[:, pl.ds(full + at, size)])
        else:
            both = dot(N[r, :], Gg[:, pl.ds(2 * full, 2 * size)])
            gate, up = both[:, :size], both[:, size:]
        H[r, pl.ds(at, size)] = (gate / (1.0 + jnp.exp(-gate)) * up).astype(BF)

    queue += [(QS, 0), (OS, 0), (G0, 0)]
    for s in range(1, half + 1):
        queue += [(QS, s), (OS, s), (G0, s)]
        if s >= half - 1:
            queue += [(G1, 0), (G2, 0)] if s == half - 1 else [(G3, 0), (E0, 0), (E1, 0)]
    for s in range(1, half + 1):
        queue += [(G1, s), (G2, s), (G3, s), (E0, s), (E1, s)]

    g0, g1, g2, g3, g4 = gather_stages(X, 0)
    local[0].wait()
    g0()
    for copy in local[1:4]:
        copy.wait()
    serve(1)
    for copy in local[4:]:
        copy.wait()
    serve(2)
    serve(3)
    g1()
    serve(3)
    g2()
    serve(3)
    g3()
    serve(3)
    g4()
    normalize(X, ag)
    serve(3)
    decay()
    serve(100 if False else 3 * (half - 5) + 5)
    serve(3)
    imported(QS)
    for t in range(4):
        project(t)
        serve(1)
    for t in range(rows // BLOCK):
        attend(t)
        serve(1)
    imported(OS)
    partial_products(M, Go, PB1)
    s0, s1, s2, s3, own = scatter_stages(PB1, D1, S1, B1, A1, 13)
    s0()
    serve(2)
    s1()
    serve(4)
    s2()
    serve(4)
    s3()

    @pl.loop(0, rows // 64)
    def _(t):
        r = pl.ds(pl.multiple_of(t * 64, 64), 64)
        F[me, r, :] = (X[me, r, :].astype(F32) + own(r)).astype(BF)

    g0, g1, g2, g3, g4 = gather_stages(F, 23)
    g0()
    serve(4)
    g1()
    serve(2)
    g2()
    serve(2)
    g3()
    serve(1)
    g4()
    normalize(F, fg)
    serve(len(queue))
    for i in (G0, G1, G2, G3):
        imported(i)
    for t in range(2):
        for at in range(0, full, 256):
            feed(t, at, min(256, full - at))
        feed(t, full, units - full)
    for i in (E0, E1):
        imported(i)
    partial_products(H, Gd, PB2)
    s0, s1, s2, s3, own = scatter_stages(PB2, D2, S2, B2, A2, 36)
    s0()
    s1()
    s2()
    s3()

    @pl.loop(0, rows // 64)
    def _(t):
        r = pl.ds(pl.multiple_of(t * 64, 64), 64)
        SS[r, :] = F[me, r, :].astype(F32) + own(r)

    second = SS[...]
    Q[me] = dot(jnp.ones((8, width), F32), second * second, ((1,), (1,)), HIGHEST)
    for k in range(1, n_tp):
        send(Q.at[me], Q.at[me], xs.at[46 + k], xr.at[46 + k], {"tp": at_tp(k)})
    for k in range(1, n_tp):
        arrived(Q.at[at_tp(-k)], xs.at[46 + k], xr.at[46 + k])
    squares = Q[0]
    for j in range(1, n_tp):
        squares = squares + Q[j]
    factor = lax.rsqrt(squares * (1.0 / d_model) + EPS)
    factor = dot(factor, jnp.full((8, width), 0.125, F32), ((0,), (0,)), HIGHEST)
    out[...] = (SS[...] * factor * fin[...]).astype(BF)

    for item in sends:
        remote(*item).wait_send()


def body(n_fs, n_tp, tokens, attn_gain, w_query, w_key, w_value, w_low, w_lift, decay_bias, head_gain,
         w_out, ffn_gain, w_gate, w_up, w_down, final_gain):
    rows, width = tokens.shape
    d_model = width * n_tp
    units = w_gate.shape[1]
    full = units // 128 * 128
    kq, ko, kd = w_query.shape[0], w_out.shape[0], w_down.shape[0]
    kd_pad = (kd + 127) // 128 * 128
    tails = jnp.concatenate([w_gate[:, full:], w_up[:, full:]], axis=1)
    any_space = pl.BlockSpec(memory_space=pl.ANY)
    vmem = pl.BlockSpec(memory_space=pltpu.VMEM)

    def scratch(*shape, dtype=BF):
        return pltpu.VMEM(shape, dtype)

    def exchange():
        return [
            scratch(n_tp, rows, width), scratch(4, rows, width), scratch(3, rows, width),
            scratch(2, rows, width), scratch(2, rows // 2, width),
        ]

    half = n_fs // 2
    n_streams = 4 + kq // 32
    ring = pltpu.SemaphoreType.DMA((n_streams, 2, half))
    return pl.pallas_call(
        functools.partial(kernel, n_fs, n_tp),
        out_shape=jax.ShapeDtypeStruct((rows, width), BF),
        in_specs=[any_space] * 9 + [vmem] * 7,
        out_specs=vmem,
        scratch_shapes=[
            scratch(n_tp, rows, width),
            scratch(d_model, 2 * DK + DV),
            scratch(n_fs, ko, 128),
            scratch(d_model, 2 * units),
            scratch(n_fs, kd_pad, 128),
            scratch(rows, d_model),
            scratch(rows, 2 * DK + DV),
            scratch(rows, DK, dtype=F32),
            scratch(rows, DV),
            scratch(n_tp, rows, width),
            scratch(rows, kd_pad),
            scratch(rows, width, dtype=F32),
            scratch(n_tp, 8, rows, dtype=F32),
            scratch(DV, DK, dtype=F32),
            *exchange(),
            *exchange(),
            pltpu.SemaphoreType.DMA((9,)),
            ring, ring, ring, ring,
            pltpu.SemaphoreType.DMA((54,)),
            pltpu.SemaphoreType.DMA((54,)),
        ],
        compiler_params=pltpu.CompilerParams(
            collective_id=0, has_side_effects=True, vmem_limit_bytes=60 * 1024 * 1024
        ),
    )(
        tokens, w_query, w_key, w_value, w_out, w_gate, w_up, tails, w_down,
        w_low, attn_gain.reshape(1, -1), w_lift, decay_bias.reshape(1, -1), head_gain.reshape(1, -1),
        ffn_gain.reshape(1, -1), final_gain.reshape(1, -1),
    )


def solution(mesh):
    n_fs, n_tp = mesh.shape["fs"], mesh.shape["tp"]
    if mesh.shape["grp"] % 2 or n_tp != 8:
        raise ValueError("unsupported mesh")
    return jax.shard_map(
        functools.partial(body, n_fs, n_tp),
        mesh=mesh,
        in_specs=(
            P(("grp", "fs"), "tp"),
            P(),
            P("fs", "tp"),
            P("fs", "tp"),
            P("fs", "tp"),
            P(),
            P(None, "tp"),
            P("tp"),
            P(),
            P("tp", "fs"),
            P(),
            P("fs", "tp"),
            P("fs", "tp"),
            P("tp", "fs"),
            P("tp"),
        ),
        out_specs=P(("grp", "fs"), "tp"),
        check_vma=False,
    )
```

```python
import functools

import jax
import jax.numpy as jnp
from jax import lax
from jax.experimental import pallas as pl
from jax.experimental.pallas import tpu as pltpu
from jax.sharding import PartitionSpec as P

DK = 128
DV = 256
BLOCK = 64
EPS = 1e-06
BF = jnp.bfloat16
F32 = jnp.float32
MESH = pl.DeviceIdType.MESH
HIGHEST = lax.Precision.HIGHEST


def dot(a, b, dims=((1,), (0,)), precision=None):
    return lax.dot_general(
        a, b, (dims, ((), ())), precision=precision, preferred_element_type=F32
    )


def kernel(
    n_fs, n_tp,
    tok, wq, wk, wv, wo, wg, wu, wd, wl, ag, wlift, bias, hg, fg,
    out,
    X, Gq, Go, Gg, Gd, N, QKV, C, M, F, H, SS, Q, state,
    PB1, D1, S1, B1, A1, T1, PB2, D2, S2, B2, A2, T2,
    lsem, zs, zr, ys, yr, xs, xr,
):
    rows, width = tok.shape
    d_model = width * n_tp
    half_rows = rows // 2
    half = n_fs // 2
    units = wg.shape[0]
    kq, ko, kd = wq.shape[0], wo.shape[0], wd.shape[0]

    grp, z, me = lax.axis_index("grp"), lax.axis_index("fs"), lax.axis_index("tp")
    parity = lax.rem(grp, 2)
    partner = {"grp": grp + 1 - 2 * parity}
    z_up, z_down = {"fs": lax.rem(z + 1, n_fs)}, {"fs": lax.rem(z + n_fs - 1, n_fs)}
    core = lax.rem(me, 2)

    def at_tp(offset):
        return lax.rem(me + offset + n_tp, n_tp)

    def other(slot):
        return slot + 1 - 2 * core

    r_slot, l_slot, o_slot = at_tp(2), at_tp(-2), at_tp(4)
    right, left, sib = {"tp": r_slot}, {"tp": l_slot}, {"tp": other(me)}

    def remote(src, dst, ssem, rsem, device):
        return pltpu.make_async_remote_copy(
            src_ref=src, dst_ref=dst, send_sem=ssem, recv_sem=rsem,
            device_id=device, device_id_type=MESH,
        )

    def send(src, dst, ssem, rsem, device):
        remote(src, dst, ssem, rsem, device).start()

    def arrived(ref, rsem):
        remote(ref, ref, xs.at[0], rsem, sib).wait_recv()

    def sent(ref, ssem):
        remote(ref, ref, ssem, xr.at[0], sib).wait_send()

    zq = pl.multiple_of(z * kq, kq)
    local = [
        (tok, X.at[me]),
        (wq, Gq.at[pl.ds(zq, kq), pl.ds(0, DK)]),
        (wk, Gq.at[pl.ds(zq, kq), pl.ds(DK, DK)]),
        (wv, Gq.at[pl.ds(zq, kq), pl.ds(2 * DK, DV)]),
        (wo, Go.at[z]),
        (wg, Gg.at[z, pl.ds(0, units), :]),
        (wu, Gg.at[z, pl.ds(units, units), :]),
        (wd, Gd.at[z, pl.ds(0, kd), :]),
    ]
    local = [pltpu.make_async_copy(s, d, lsem.at[i]) for i, (s, d) in enumerate(local)]
    for copy in local:
        copy.start()

    barrier = pltpu.get_barrier_semaphore()
    greeted = [z_up, z_down, partner] + [{"tp": at_tp(k)} for k in range(1, n_tp)]
    for device in greeted:
        pl.semaphore_signal(barrier, inc=1, device_id=device, device_id_type=MESH)
    if kd < Gd.shape[1]:
        Gd[:, kd:, :] = jnp.zeros((n_fs, Gd.shape[1] - kd, 128), BF)
        H[:, units:] = jnp.zeros((rows, H.shape[1] - units), BF)
    pl.semaphore_wait(barrier, len(greeted))

    def by_rows(view, base, total, edge):
        chunk, other_edge = total - edge, total - edge

        def part(shard, start, size):
            return view(shard, pl.multiple_of(base + start, 16), size)

        first = (chunk // 2 + 15) // 16 * 16
        return dict(
            ring=lambda s: part(s, parity * edge, chunk),
            mine=lambda s: part(s, parity * other_edge, edge),
            theirs=lambda s: part(s, (1 - parity) * other_edge, edge),
            sizes=(chunk, edge),
            halves=(
                lambda s: part(s, parity * edge, first),
                lambda s: part(s, parity * edge + first, chunk - first),
            ),
        )

    def view_q(shard, start, size):
        return Gq.at[pl.ds(pl.multiple_of(shard * kq + start, 16), size), :]

    def view_of(G):
        return lambda shard, start, size: G.at[shard, pl.ds(start, size), :]

    half_q, half_d = kq // 2, kd // 2
    streams = [
        by_rows(view_q, 0, half_q, 16),
        by_rows(view_q, half_q, half_q, 32),
        by_rows(view_of(Go), 0, ko, 80),
    ]
    streams += [by_rows(view_of(Gg), k * half_d, half_d, 112 if k % 2 == 0 else 96) for k in range(4)]
    streams += [by_rows(view_of(Gd), k * half_d, half_d, 96) for k in range(2)]
    QA, QB, OS, G0, G1, U0, U1, E0, E1 = range(9)

    def launch(i):
        ref = streams[i]["ring"](z)
        send(ref, ref, zs.at[i], zr.at[i, 0, 0], z_up)
        send(ref, ref, zs.at[i], zr.at[i, 1, 0], z_down)

    def event(i, s):
        st = streams[i]
        for way, (shard, device) in enumerate(
            ((lax.rem(z - s + n_fs, n_fs), z_up), (lax.rem(z + s, n_fs), z_down))
        ):
            if s < half:
                arrived(st["ring"](shard), zr.at[i, way, s - 1])
                ref = st["ring"](shard) if s + 1 < half else st["halves"][way](shard)
                send(ref, ref, zs.at[i], zr.at[i, way, s], device)
            else:
                arrived(st["halves"][way](shard), zr.at[i, way, s - 1])
            if s < half or way == 1:
                ref = st["mine"](shard)
                send(ref, ref, ys.at[i], yr.at[i], partner)

    def others(size):
        return Gg.at[pl.ds(0, n_fs - 1), pl.ds(0, size), :]

    def lanes(i):
        return 4 if i in (QA, QB) else 1

    def imported(i):
        arrived(others(streams[i]["sizes"][1] * lanes(i)), yr.at[i])

    queue = []

    def serve(count):
        while queue and (count or queue[0][1] == 0):
            item = queue.pop(0)
            if item[1] == 0:
                launch(item[0])
            else:
                event(*item)
                count -= 1

    def serve_to(*item):
        serve(sum(step > 0 for _, step in queue[: queue.index(item) + 1]))

    top, low = pl.ds(0, half_rows), pl.ds(half_rows, half_rows)

    def gather_stages(buf, base, family):
        def go(k, slot, part, device):
            ref = buf.at[slot] if part is None else buf.at[slot, part, :]
            send(ref, ref, xs.at[family], xr.at[base + k], device)

        def got(k, slot, part):
            ref = buf.at[slot] if part is None else buf.at[slot, part, :]
            arrived(ref, xr.at[base + k])

        def s0():
            go(0, me, top, right)
            go(2, me, low, left)
            go(1, me, low, right)
            go(3, me, top, left)
            go(4, me, None, sib)

        def s1():
            got(0, l_slot, top)
            go(5, l_slot, top, right)
            go(6, l_slot, top, sib)
            got(2, r_slot, low)
            go(7, r_slot, low, left)
            go(8, r_slot, low, sib)

        def s2():
            got(1, l_slot, low)
            go(9, l_slot, low, sib)
            got(3, r_slot, top)
            go(10, r_slot, top, sib)

        def s3():
            got(5, o_slot, top)
            go(11, o_slot, top, sib)
            got(7, o_slot, low)
            go(12, o_slot, low, sib)

        def s4():
            got(4, other(me), None)
            got(6, other(l_slot), top)
            got(8, other(r_slot), low)
            got(9, other(l_slot), low)
            got(10, other(r_slot), top)
            got(11, other(o_slot), top)
            got(12, other(o_slot), low)

        return s0, s1, s2, s3, s4

    def scatter_stages(left_ref, G, PB, D, S, B, A, T, SS, base, family):
        def go(k, src, dst, device):
            send(src, dst, xs.at[family], xr.at[base + k], device)

        def got(k, dst):
            arrived(dst, xr.at[base + k])

        def product(slot, part):
            weight = jnp.concatenate([G[2 * slot], G[2 * slot + 1]], axis=1)
            return dot(left_ref[part, :], weight)

        def s0(k):
            slot = other((o_slot, r_slot, l_slot, me)[k])
            for part in (top, low):
                PB[k, part, :] = product(slot, part).astype(BF)
            go(k, PB.at[k], D.at[k], sib)

        def s1(k):
            slot = (o_slot, r_slot, l_slot, me)[k]
            parts = [product(slot, part) for part in (top, low)]
            got(k, D.at[k])
            parts = [p + D[k, part, :].astype(F32) for p, part in zip(parts, (top, low))]
            if k == 0:
                S[0, top, :] = parts[0].astype(BF)
                go(4, S.at[0, top, :], A.at[0], right)
                S[0, low, :] = parts[1].astype(BF)
                go(5, S.at[0, low, :], A.at[1], left)
            elif k == 1:
                S[1, low, :] = parts[1].astype(BF)
                go(6, S.at[1, low, :], B.at[0, low, :], right)
                T[0] = parts[0]
            elif k == 2:
                S[2, top, :] = parts[0].astype(BF)
                go(7, S.at[2, top, :], B.at[1, top, :], left)
                T[1] = parts[1]
            else:
                SS[top, :] = parts[0]
                SS[low, :] = parts[1]

        def s2():
            got(4, A.at[0])
            S[1, top, :] = (T[0] + A[0].astype(F32)).astype(BF)
            go(8, S.at[1, top, :], B.at[0, top, :], right)
            got(5, A.at[1])
            S[2, low, :] = (T[1] + A[1].astype(F32)).astype(BF)
            go(9, S.at[2, low, :], B.at[1, low, :], left)

        def s3():
            got(6, B.at[0, low, :])
            got(7, B.at[1, top, :])
            got(8, B.at[0, top, :])
            got(9, B.at[1, low, :])

        def own(r):
            return SS[r, :] + B[0, r, :].astype(F32) + B[1, r, :].astype(F32)

        return s0, s1, s2, s3, own

    def normalize(buf, gain):
        step = 32

        @pl.loop(0, rows // step)
        def _(t):
            r = pl.ds(pl.multiple_of(t * step, step), step)
            blocks = [buf[j, r, :].astype(F32) for j in range(n_tp)]
            squares = blocks[0] * blocks[0]
            for b in blocks[1:]:
                squares = squares + b * b
            factor = lax.rsqrt(jnp.sum(squares, axis=1, keepdims=True) * (1.0 / d_model) + EPS)
            for j, b in enumerate(blocks):
                cols = pl.ds(j * width, width)
                N[r, cols] = (b * factor * gain[:, cols]).astype(BF)

    ti = lax.broadcasted_iota(jnp.int32, (BLOCK, BLOCK), 0)
    si = lax.broadcasted_iota(jnp.int32, (BLOCK, BLOCK), 1)

    def decay(part):
        tril = jnp.where(ti >= si, 1.0, 0.0).astype(BF)
        step = 2 * BLOCK

        @pl.loop(part * (rows // step // 2), (part + 1) * (rows // step // 2))
        def _(t):
            r = pl.ds(pl.multiple_of(t * step, step), step)
            rank = dot(N[r, :], wl[...], ((1,), (1,))).astype(BF)
            v = dot(rank, wlift[...]) + bias[...]
            log_decay = (jnp.minimum(v, 0.0) - jnp.log1p(jnp.exp(-jnp.abs(v)))) * (1.0 / 16.0)
            for k in range(2):
                part = log_decay[k * BLOCK : (k + 1) * BLOCK]
                hi = part.astype(BF)
                lo = (part - hi.astype(F32)).astype(BF)
                r2 = pl.ds(pl.multiple_of(t * step + k * BLOCK, BLOCK), BLOCK)
                C[r2, :] = dot(tril, hi) + dot(tril, lo)

    def project(t):
        step = rows // 4
        r = pl.ds(t * step, step)
        QKV[r, :] = dot(N[r, :], Gq[...]).astype(BF)

    def attend(t):
        r = pl.ds(t * BLOCK, BLOCK)
        c = C[r, :]
        last = C[pl.ds((t + 1) * BLOCK - 1, 1), :]
        q = QKV[r, pl.ds(0, DK)].astype(F32) * DK ** (-0.5)
        k = QKV[r, pl.ds(DK, DK)].astype(F32)
        v = QKV[r, pl.ds(2 * DK, DV)]
        q_dec = (q * jnp.exp(c)).astype(BF)
        k_dec = (k * jnp.exp(-c)).astype(BF)
        k_end = (k * jnp.exp(last - c)).astype(BF)
        scores = jnp.where(ti >= si, dot(q_dec, k_dec, ((1,), (1,))), 0.0).astype(BF)
        o = dot(scores, v)
        if t > 0:
            o = o + dot(q_dec, state[...].astype(BF), ((1,), (1,)))
        added = dot(v, k_end, ((0,), (0,)))
        state[...] = state[...] * jnp.exp(last) + added if t > 0 else added
        factor = lax.rsqrt(jnp.mean(o * o, axis=1, keepdims=True) + EPS)
        M[r, :] = (o * factor * hg[...]).astype(BF)

    def feed(t, at, size):
        step = rows // 2
        r = pl.ds(t * step, step)

        def product(start):
            weight = jnp.concatenate([Gg[j, pl.ds(start, size), :] for j in range(n_fs)], axis=1)
            return dot(N[r, :], weight, ((1,), (1,)))

        gate, up = product(at), product(units + at)
        H[r, pl.ds(at, size)] = (gate / (1.0 + jnp.exp(-gate)) * up).astype(BF)

    queue += [(QA, 0), (QB, 0), (OS, 0), (G0, 0)]
    for s in range(1, half + 1):
        queue += [(QA, s), (QB, s), (OS, s), (G0, s)]
        if s == half - 1:
            queue += [(U0, 0), (G1, 0)]
        if s == half:
            queue += [(U1, 0)]
    for s in range(1, half + 1):
        queue += [(U0, s), (G1, s), (U1, s)]
        if s == 1:
            queue += [(E0, 0), (E1, 0)]
        if s > 1:
            queue += [(E0, s - 1), (E1, s - 1)]
    queue += [(E0, half), (E1, half)]

    g0, g1, g2, g3, g4 = gather_stages(X, 0, 0)
    local[0].wait()
    g0()
    for copy in local[1:]:
        copy.wait()
    serve_to(OS, 1)
    g1()
    serve_to(OS, 2)
    g2()
    serve_to(OS, 3)
    g3()
    serve_to(OS, 4)
    g4()
    normalize(X, ag)
    serve_to(OS, 5)
    decay(0)
    serve_to(OS, 6)
    decay(1)
    serve_to(OS, half)
    serve(2)
    imported(QA)
    imported(QB)
    for t in range(4):
        project(t)
        if t % 2:
            serve(1)
    for t in range(rows // BLOCK):
        attend(t)
        if t in (2, 5):
            serve(1)
    imported(OS)
    s0, s1, s2, s3, own = scatter_stages(M, Go, PB1, D1, S1, B1, A1, T1, SS, 13, 1)
    for k in range(4):
        s0(k)
    serve(1)
    for k in range(4):
        s1(k)
    serve(5)
    s2()
    serve(5)
    s3()

    @pl.loop(0, rows // 64)
    def _(t):
        r = pl.ds(pl.multiple_of(t * 64, 64), 64)
        F[me, r, :] = (X[me, r, :].astype(F32) + own(r)).astype(BF)

    g0, g1, g2, g3, g4 = gather_stages(F, 23, 2)
    g0()
    serve(6)
    g1()
    serve(3)
    g2()
    serve(2)
    g3()
    serve(1)
    g4()
    normalize(F, fg)
    serve_to(U1, half)
    for i in (G0, U0, G1, U1):
        imported(i)
    for t in range(2):
        for at in range(0, units, 256):
            feed(t, at, min(256, units - at))
            serve(1)
    serve(1000)
    for i in (E0, E1):
        imported(i)
    s0, s1, s2, s3, own = scatter_stages(H, Gd, PB2, D2, S2, B2, A2, T2, SS, 36, 3)
    for k in range(4):
        s0(k)
    for k in range(4):
        s1(k)
    s2()
    s3()

    ones = jnp.ones((8, width), BF)

    def in_two(v):
        hi = v.astype(BF)
        return hi, (v - hi.astype(F32)).astype(BF)

    with jax.named_scope("second"):
        for part in (top, low):
            second = F[me, part, :].astype(F32) + own(part)
            SS[part, :] = second
            Q[me, :, part] = sum(dot(ones, v, ((1,), (1,))) for v in in_two(second * second))
    with jax.named_scope("squares"):
        for k in range(1, n_tp):
            send(Q.at[me], Q.at[me], xs.at[4], xr.at[46 + k], {"tp": at_tp(k)})
        for k in range(1, n_tp):
            arrived(Q.at[at_tp(-k)], xr.at[46 + k])
    with jax.named_scope("close"):
        squares = Q[0]
        for j in range(1, n_tp):
            squares = squares + Q[j]
        eighth = jnp.full((8, width), 0.125, BF)
        factors = in_two(lax.rsqrt(squares * (1.0 / d_model) + EPS))
        for part in (0, half_rows):
            factor = sum(dot(v[:, part : part + half_rows], eighth, ((0,), (0,))) for v in factors)
            out[pl.ds(part, half_rows), :] = SS[pl.ds(part, half_rows), :] * factor
    with jax.named_scope("drain"):
        for i, st in enumerate(streams):
            sent(others(st["sizes"][0] * lanes(i)), zs.at[i])
            sent(others(st["sizes"][1] * lanes(i)), ys.at[i])
        for family in range(4):
            sent(X.at[pl.ds(0, n_tp - 1)], xs.at[family])
        sent(Q.at[pl.ds(0, n_tp - 1)], xs.at[4])


def body(n_fs, n_tp, tokens, attn_gain, w_query, w_key, w_value, w_low, w_lift, decay_bias, head_gain,
         w_out, ffn_gain, w_gate, w_up, w_down, final_gain):
    rows, width = tokens.shape
    d_model = width * n_tp
    units = w_gate.shape[1]
    kq, ko, kd = w_query.shape[0], w_out.shape[0], w_down.shape[0]
    kd_pad = (kd + 127) // 128 * 128
    any_space = pl.BlockSpec(memory_space=pl.ANY)
    vmem = pl.BlockSpec(memory_space=pltpu.VMEM)

    def scratch(*shape, dtype=BF):
        return pltpu.VMEM(shape, dtype)

    def exchange():
        return [
            scratch(4, rows, width), scratch(4, rows, width), scratch(3, rows, width),
            scratch(2, rows, width), scratch(2, rows // 2, width), scratch(2, rows // 2, width, dtype=F32),
        ]

    half = n_fs // 2
    n_streams = 9
    ring = pltpu.SemaphoreType.DMA((n_streams, 2, half))
    per_stream = pltpu.SemaphoreType.DMA((n_streams,))
    result = pl.pallas_call(
        functools.partial(kernel, n_fs, n_tp),
        out_shape=jax.ShapeDtypeStruct((rows, width), F32),
        in_specs=[any_space] * 8 + [vmem] * 6,
        out_specs=vmem,
        scratch_shapes=[
            scratch(n_tp, rows, width),
            scratch(d_model, 2 * DK + DV),
            scratch(n_fs, ko, 128),
            scratch(n_fs, 2 * units, 128),
            scratch(n_fs, kd_pad, 128),
            scratch(rows, d_model),
            scratch(rows, 2 * DK + DV),
            scratch(rows, DK, dtype=F32),
            scratch(rows, DV),
            scratch(n_tp, rows, width),
            scratch(rows, kd_pad),
            scratch(rows, width, dtype=F32),
            scratch(n_tp, 8, rows, dtype=F32),
            scratch(DV, DK, dtype=F32),
            *exchange(),
            *exchange(),
            pltpu.SemaphoreType.DMA((8,)),
            per_stream, ring, per_stream, per_stream,
            pltpu.SemaphoreType.DMA((5,)),
            pltpu.SemaphoreType.DMA((54,)),
        ],
        compiler_params=pltpu.CompilerParams(
            collective_id=0, has_side_effects=True, vmem_limit_bytes=67043328
        ),
    )(
        tokens, w_query, w_key, w_value, w_out, w_gate.T, w_up.T, w_down,
        w_low.T, attn_gain.reshape(1, -1), w_lift, decay_bias.reshape(1, -1), head_gain.reshape(1, -1),
        ffn_gain.reshape(1, -1),
    )
    return (result * final_gain).astype(BF)


def solution(mesh):
    n_fs, n_tp = mesh.shape["fs"], mesh.shape["tp"]
    if mesh.shape["grp"] % 2 or n_tp != 8:
        raise ValueError("unsupported mesh")
    return jax.shard_map(
        functools.partial(body, n_fs, n_tp),
        mesh=mesh,
        in_specs=(
            P(("grp", "fs"), "tp"),
            P(),
            P("fs", "tp"),
            P("fs", "tp"),
            P("fs", "tp"),
            P(),
            P(None, "tp"),
            P("tp"),
            P(),
            P("tp", "fs"),
            P(),
            P("fs", "tp"),
            P("fs", "tp"),
            P("tp", "fs"),
            P("tp"),
        ),
        out_specs=P(("grp", "fs"), "tp"),
        check_vma=False,
    )
```

```python
import functools

import jax
import jax.numpy as jnp
from jax import lax
from jax.experimental import pallas as pl
from jax.experimental.pallas import tpu as pltpu
from jax.sharding import PartitionSpec as P

DK = 128
DV = 256
BLOCK = 64
EPS = 1e-06
START, LATENCY, RATE = 2.3, 2.6, 46.6e3
BF = jnp.bfloat16
F32 = jnp.float32
MESH = pl.DeviceIdType.MESH
HIGHEST = lax.Precision.HIGHEST


def dot(a, b, dims=((1,), (0,)), precision=None):
    return lax.dot_general(
        a, b, (dims, ((), ())), precision=precision, preferred_element_type=F32
    )


def kernel(
    n_fs, n_tp,
    tok, wq, wk, wv, wo, wg, wu, wd, wl_in, ag_in, wlift_in, bias_in, hg_in, fg_in, fin_in,
    out,
    wl, ag, wlift, bias, hg, fg, fin,
    X, Gq, Go, Gg, Gd, N, QKV, C, M, F, H, SS, Q, state,
    PB1, D1, S1, B1, A1, T1, PB2, D2, S2, B2, A2, T2,
    lsem, zs, zr, ys, yr, xs, xr,
):
    rows, width = tok.shape
    d_model = width * n_tp
    half_rows = rows // 2
    half = n_fs // 2
    units = wg.shape[0]
    kq, ko, kd = wq.shape[0], wo.shape[0], wd.shape[0]

    grp, z, me = lax.axis_index("grp"), lax.axis_index("fs"), lax.axis_index("tp")
    parity = lax.rem(grp, 2)
    partner = {"grp": grp + 1 - 2 * parity}
    z_up, z_down = {"fs": lax.rem(z + 1, n_fs)}, {"fs": lax.rem(z + n_fs - 1, n_fs)}
    core = lax.rem(me, 2)

    def at_tp(offset):
        return lax.rem(me + offset + n_tp, n_tp)

    def other(slot):
        return slot + 1 - 2 * core

    r_slot, l_slot, o_slot = at_tp(2), at_tp(-2), at_tp(4)
    right, left, sib = {"tp": r_slot}, {"tp": l_slot}, {"tp": other(me)}

    def remote(src, dst, ssem, rsem, device):
        return pltpu.make_async_remote_copy(
            src_ref=src, dst_ref=dst, send_sem=ssem, recv_sem=rsem,
            device_id=device, device_id_type=MESH,
        )

    def send(src, dst, ssem, rsem, device):
        remote(src, dst, ssem, rsem, device).start()

    def arrived(ref, rsem):
        remote(ref, ref, xs.at[0], rsem, sib).wait_recv()

    def sent(ref, ssem):
        remote(ref, ref, ssem, xr.at[0], sib).wait_send()

    barrier = pltpu.get_barrier_semaphore()
    greeted = [z_up, z_down, partner] + [{"tp": at_tp(k)} for k in range(1, n_tp)]
    for device in greeted:
        pl.semaphore_signal(barrier, inc=1, device_id=device, device_id_type=MESH)
    zq = pl.multiple_of(z * kq, kq)
    local = [
        (tok, X.at[me]),
        (wq, Gq.at[pl.ds(zq, kq), pl.ds(0, DK)]),
        (wk, Gq.at[pl.ds(zq, kq), pl.ds(DK, DK)]),
        (wv, Gq.at[pl.ds(zq, kq), pl.ds(2 * DK, DV)]),
        (wo, Go.at[z]),
        (wg, Gg.at[z, pl.ds(0, units), :]),
        (wu, Gg.at[z, pl.ds(units, units), :]),
        (wd, Gd.at[z, pl.ds(0, kd), :]),
    ]
    local = [pltpu.make_async_copy(s, d, lsem.at[i]) for i, (s, d) in enumerate(local)]
    for copy in local:
        copy.start()

    small = [(wl_in, wl), (ag_in, ag), (wlift_in, wlift), (bias_in, bias), (hg_in, hg), (fg_in, fg), (fin_in, fin)]
    small = [pltpu.make_async_copy(s, d, lsem.at[8 + i]) for i, (s, d) in enumerate(small)]
    for copy in small:
        copy.start()

    if kd < Gd.shape[1]:
        Gd[:, kd:, :] = jnp.zeros((n_fs, Gd.shape[1] - kd, 128), BF)
        H[:, units:] = jnp.zeros((rows, H.shape[1] - units), BF)
    pl.semaphore_wait(barrier, len(greeted))

    def by_rows(view, base, total, edge):
        chunk, other_edge = total - edge, total - edge

        def part(shard, start, size):
            return view(shard, pl.multiple_of(base + start, 16), size)

        first = (chunk // 2 + 15) // 16 * 16
        return dict(
            ring=lambda s: part(s, parity * edge, chunk),
            mine=lambda s: part(s, parity * other_edge, edge),
            theirs=lambda s: part(s, (1 - parity) * other_edge, edge),
            sizes=(chunk, edge),
            halves=(
                lambda s: part(s, parity * edge, first),
                lambda s: part(s, parity * edge + first, chunk - first),
            ),
        )

    def view_q(shard, start, size):
        return Gq.at[pl.ds(pl.multiple_of(shard * kq + start, 16), size), :]

    def view_of(G):
        return lambda shard, start, size: G.at[shard, pl.ds(start, size), :]

    half_q, half_d, tail = kq // 2, kd // 2, units - 2 * 256
    streams = [
        by_rows(view_q, 0, half_q, 16),
        by_rows(view_q, half_q, half_q, 32),
        by_rows(view_of(Go), 0, ko, 80),
        by_rows(view_of(Gg), 0, 256, 80),
        by_rows(view_of(Gg), units, 256, 80),
        by_rows(view_of(Gg), 256, 256, 80),
        by_rows(view_of(Gg), units + 256, 256, 80),
        by_rows(view_of(Gg), 512, tail, 80),
        by_rows(view_of(Gg), units + 512, tail, 80),
        by_rows(view_of(Gd), 0, half_d, 96),
        by_rows(view_of(Gd), half_d, half_d, 96),
    ]
    QA, QB, OS, G0, U0, G1, U1, G2, U2, E0, E1 = range(11)

    def launch(i):
        ref = streams[i]["ring"](z)
        send(ref, ref, zs.at[i], zr.at[i, 0], z_up)
        send(ref, ref, zs.at[i], zr.at[i, 0], z_down)

    def event(i, s):
        st = streams[i]
        flows = ((lax.rem(z - s + n_fs, n_fs), z_up), (lax.rem(z + s, n_fs), z_down))
        arrived(some(1 if s == half else 2, st["sizes"][0] * lanes(i)), zr.at[i, s - 1])
        for way, (shard, device) in enumerate(flows):
            if s < half:
                ref = st["ring"](shard) if s + 1 < half else st["halves"][way](shard)
                send(ref, ref, zs.at[i], zr.at[i, s], device)
        for way, (shard, device) in enumerate(flows):
            if s < half or way == 1:
                ref = st["mine"](shard)
                send(ref, ref, ys.at[i], yr.at[i], partner)

    def some(shards, size):
        return Gg.at[pl.ds(0, shards), pl.ds(0, size), :]

    def others(size):
        return some(n_fs - 1, size)

    def lanes(i):
        return 4 if i in (QA, QB) else 1

    def imported(*which):
        for i in which:
            arrived(others(streams[i]["sizes"][1] * lanes(i)), yr.at[i])

    queue = []

    left_at, clock, link = {}, [START], [START]

    def due(until=None):
        until = clock[0] if until is None else until
        while queue:
            i, s = queue[0]
            arrival = left_at[i, s - 1] + LATENCY if s else clock[0]
            if arrival > until:
                break
            queue.pop(0)
            with jax.named_scope("ev%d_%d" % (i, s)):
                if s == 0:
                    launch(i)
                else:
                    event(i, s)
            clock[0] = max(clock[0], arrival) + (0.1 if s else 0.0)
            if s < half:
                weight = streams[i]["sizes"][0] * lanes(i) * 256 / RATE
                link[0] = max(link[0], clock[0]) + weight * (0.5 if s == half - 1 else 1)
                left_at[i, s] = link[0]
        clock[0] = max(clock[0], min(until, 1000.0))

    def due_to(*item):
        while item in queue:
            i, s = queue[0]
            due(left_at[i, s - 1] + LATENCY if s else clock[0])

    def work(us):
        clock[0] += us
        due()

    top, low = pl.ds(0, half_rows), pl.ds(half_rows, half_rows)

    def gather_stages(buf, base, family):
        def go(k, slot, part, device):
            ref = buf.at[slot] if part is None else buf.at[slot, part, :]
            send(ref, ref, xs.at[family], xr.at[base + k], device)

        def got(k, slot, part):
            ref = buf.at[slot] if part is None else buf.at[slot, part, :]
            arrived(ref, xr.at[base + k])

        def s0():
            go(0, me, top, right)
            go(2, me, low, left)
            go(1, me, low, right)
            go(3, me, top, left)
            go(4, me, None, sib)

        def s1():
            got(0, l_slot, top)
            go(5, l_slot, top, right)
            go(6, l_slot, top, sib)
            got(2, r_slot, low)
            go(7, r_slot, low, left)
            go(8, r_slot, low, sib)

        def s2():
            got(1, l_slot, low)
            go(9, l_slot, low, sib)
            got(3, r_slot, top)
            go(10, r_slot, top, sib)

        def s3():
            got(5, o_slot, top)
            go(11, o_slot, top, sib)
            got(7, o_slot, low)
            go(12, o_slot, low, sib)

        def s4():
            got(4, other(me), None)
            got(6, other(l_slot), top)
            got(8, other(r_slot), low)
            got(9, other(l_slot), low)
            got(10, other(r_slot), top)
            got(11, other(o_slot), top)
            got(12, other(o_slot), low)

        return s0, s1, s2, s3, s4

    def scatter_stages(left_ref, G, PB, D, S, B, A, T, SS, base, family):
        def go(k, src, dst, device):
            send(src, dst, xs.at[family], xr.at[base + k], device)

        def got(k, dst):
            arrived(dst, xr.at[base + k])

        def product(slot, part):
            weight = jnp.concatenate([G[2 * slot], G[2 * slot + 1]], axis=1)
            return dot(left_ref[part, :], weight)

        def quarter(q):
            return pl.ds(q * (half_rows // 2), half_rows // 2)

        def s0(k):
            slot = other((o_slot, r_slot, l_slot, me)[k])
            for part in (top, low):
                PB[k, part, :] = product(slot, part).astype(BF)
            go(k, PB.at[k], D.at[k], sib)

        def s1(k):
            slot = (o_slot, r_slot, l_slot, me)[k]
            parts = [product(slot, part) for part in (top, low)]
            got(k, D.at[k])
            parts = [p + D[k, part, :].astype(F32) for p, part in zip(parts, (top, low))]
            if k == 0:
                for way in range(2):
                    S[0, (top, low)[way], :] = parts[way].astype(BF)
                for h in range(2):
                    for way in range(2):
                        src = S.at[0, quarter(2 * way + h), :]
                        go((4, 10, 5, 11)[2 * way + h], src, A.at[way, quarter(h), :], (right, left)[way])
            elif k == 1:
                S[1, low, :] = parts[1].astype(BF)
                go(6, S.at[1, low, :], B.at[0, low, :], right)
                T[0] = parts[0]
            elif k == 2:
                S[2, top, :] = parts[0].astype(BF)
                go(7, S.at[2, top, :], B.at[1, top, :], left)
                T[1] = parts[1]
            else:
                SS[top, :] = parts[0]
                SS[low, :] = parts[1]

        def s2(h):
            for way in range(2):
                q = quarter(2 * way + h)
                got((4, 10, 5, 11)[2 * way + h], A.at[way, quarter(h), :])
                S[1 + way, q, :] = (T[way, quarter(h), :] + A[way, quarter(h), :].astype(F32)).astype(BF)
                go((8, 12, 9, 13)[2 * way + h], S.at[1 + way, q, :], B.at[way, q, :], (right, left)[way])

        def s3():
            got(6, B.at[0, low, :])
            got(7, B.at[1, top, :])
            for k, way, q in ((8, 0, 0), (9, 1, 2), (12, 0, 1), (13, 1, 3)):
                got(k, B.at[way, quarter(q), :])

        def own(r):
            return SS[r, :] + B[0, r, :].astype(F32) + B[1, r, :].astype(F32)

        return s0, s1, s2, s3, own

    def normalize(buf, gain, part):
        step = 32

        @pl.loop(part * (rows // step // 4), (part + 1) * (rows // step // 4))
        def _(t):
            r = pl.ds(pl.multiple_of(t * step, step), step)
            blocks = [buf[j, r, :].astype(F32) for j in range(n_tp)]
            squares = blocks[0] * blocks[0]
            for b in blocks[1:]:
                squares = squares + b * b
            factor = lax.rsqrt(jnp.sum(squares, axis=1, keepdims=True) * (1.0 / d_model) + EPS)
            for j, b in enumerate(blocks):
                cols = pl.ds(j * width, width)
                N[r, cols] = (b * factor * gain[:, cols]).astype(BF)

    ti = lax.broadcasted_iota(jnp.int32, (BLOCK, BLOCK), 0)
    si = lax.broadcasted_iota(jnp.int32, (BLOCK, BLOCK), 1)

    def decay(part):
        tril = jnp.where(ti >= si, 1.0, 0.0).astype(BF)
        step = 2 * BLOCK

        @pl.loop(part * (rows // step // 4), (part + 1) * (rows // step // 4))
        def _(t):
            r = pl.ds(pl.multiple_of(t * step, step), step)
            rank = dot(N[r, :], wl[...], ((1,), (1,))).astype(BF)
            v = dot(rank, wlift[...]) + bias[...]
            log_decay = (jnp.minimum(v, 0.0) - jnp.log1p(jnp.exp(-jnp.abs(v)))) * (1.0 / 16.0)
            for k in range(2):
                part = log_decay[k * BLOCK : (k + 1) * BLOCK]
                hi = part.astype(BF)
                lo = (part - hi.astype(F32)).astype(BF)
                r2 = pl.ds(pl.multiple_of(t * step + k * BLOCK, BLOCK), BLOCK)
                C[r2, :] = dot(tril, hi) + dot(tril, lo)

    def project(t):
        step = rows // 4
        r = pl.ds(t * step, step)
        QKV[r, :] = dot(N[r, :], Gq[...]).astype(BF)

    def attend(t):
        r = pl.ds(t * BLOCK, BLOCK)
        c = C[r, :]
        last = C[pl.ds((t + 1) * BLOCK - 1, 1), :]
        q = QKV[r, pl.ds(0, DK)].astype(F32) * DK ** (-0.5)
        k = QKV[r, pl.ds(DK, DK)].astype(F32)
        v = QKV[r, pl.ds(2 * DK, DV)]
        q_dec = (q * jnp.exp(c)).astype(BF)
        k_dec = (k * jnp.exp(-c)).astype(BF)
        k_end = (k * jnp.exp(last - c)).astype(BF)
        scores = jnp.where(ti >= si, dot(q_dec, k_dec, ((1,), (1,))), 0.0).astype(BF)
        o = dot(scores, v)
        if t > 0:
            o = o + dot(q_dec, state[...].astype(BF), ((1,), (1,)))
        added = dot(v, k_end, ((0,), (0,)))
        state[...] = state[...] * jnp.exp(last) + added if t > 0 else added
        factor = lax.rsqrt(jnp.mean(o * o, axis=1, keepdims=True) + EPS)
        M[r, :] = (o * factor * hg[...]).astype(BF)

    def feed(t, at, size):
        step = rows // 2
        r = pl.ds(t * step, step)

        def product(start):
            weight = jnp.concatenate([Gg[j, pl.ds(start, size), :] for j in range(n_fs)], axis=1)
            return dot(N[r, :], weight, ((1,), (1,)))

        gate, up = product(at), product(units + at)
        H[r, pl.ds(at, size)] = (gate / (1.0 + jnp.exp(-gate)) * up).astype(BF)

    plan = (((QA, QB, OS, G0), 0), ((U0, G1, U1), 6), ((G2, U2), 7), ((E0, E1), 8))
    for r in range(half + 9):
        for group, start in plan:
            if 0 <= r - start <= half:
                queue += [(i, r - start) for i in group]

    def gather(buf, base, family):
        g0, g1, g2, g3, g4 = gather_stages(buf, base, family)
        g0()
        begun = clock[0]
        for stage, ready in ((g1, 5.1), (g2, 7.8), (g3, 10.3), (g4, 11.1)):
            due(begun + ready - 0.2)
            stage()
            work(0.1)

    def scatter(stages):
        s0, s1, s2, s3, own = stages
        for k in range(3):
            s0(k)
            work(0.25)
        begun = clock[0] + 0.3
        s1(0)
        s0(3)
        work(0.6)
        for k in range(1, 4):
            s1(k)
            work(0.27)
        due(begun + 4.2)
        s2(0)
        work(0.1)
        due(begun + 5.4)
        s2(1)
        work(0.1)
        due(begun + 10.0)
        s3()
        return own

    local[0].wait()
    for copy in local[1:]:
        copy.wait()
    due()
    gather(X, 0, 0)
    for copy in small:
        copy.wait()
    for t in range(4):
        normalize(X, ag, t)
        work(0.55)
    for t in range(4):
        decay(t)
        work(0.6)
    due_to(QB, half)
    due(clock[0] + 3.0)
    imported(QA, QB)
    for t in range(4):
        project(t)
        work(0.37)
    for t in range(rows // BLOCK):
        attend(t)
        work(0.2)
    imported(OS)
    own = scatter(scatter_stages(M, Go, PB1, D1, S1, B1, A1, T1, SS, 13, 1))

    @pl.loop(0, rows // 64)
    def _(t):
        r = pl.ds(pl.multiple_of(t * 64, 64), 64)
        F[me, r, :] = (X[me, r, :].astype(F32) + own(r)).astype(BF)

    work(0.3)
    gather(F, 27, 2)
    for t in range(4):
        normalize(F, fg, t)
        work(0.55)
    due_to(E1, half - 2)
    imported(G0, U0, G1, U1)
    feed(0, 0, 256)
    feed(0, 256, 256)
    feed(1, 0, 256)
    clock[0] += 2.3
    due_to(E1, half - 1)
    feed(1, 256, 256)
    imported(G2, U2)
    for t in range(2):
        feed(t, 512, units - 512)
    clock[0] += 2.3
    due(10000.0)
    imported(E0, E1)
    own = scatter(scatter_stages(H, Gd, PB2, D2, S2, B2, A2, T2, SS, 40, 3))

    ones = jnp.ones((8, width), BF)
    row = lax.broadcasted_iota(jnp.int32, (8, 128), 0)

    def in_two(v):
        hi = v.astype(BF)
        return hi, (v - hi.astype(F32)).astype(BF)

    with jax.named_scope("second"):
        packed = jnp.zeros((8, 128), F32)
        for b in range(rows // 128):
            part = pl.ds(b * 128, 128)
            second = F[me, part, :].astype(F32) + own(part)
            SS[part, :] = second
            sums = sum(dot(ones, v, ((1,), (1,))) for v in in_two(second * second))
            packed = jnp.where(row == b, sums, packed)
        Q[me] = packed
    with jax.named_scope("squares"):
        for k in (4, 5, 3, 2, 6, 7, 1):
            send(Q.at[me], Q.at[me], xs.at[4], xr.at[53 + k], {"tp": at_tp(k)})
        for k in range(1, n_tp):
            arrived(Q.at[at_tp(-k)], xr.at[53 + k])
    with jax.named_scope("close"):
        squares = Q[0]
        for j in range(1, n_tp):
            squares = squares + Q[j]
        factors = lax.rsqrt(squares * (1.0 / d_model) + EPS)
        for b in range(rows // 128):
            part = pl.ds(b * 128, 128)
            factor = sum(
                dot(v, ones, ((0,), (0,))) for v in in_two(jnp.where(row == b, factors, 0.0))
            )
            out[part, :] = (SS[part, :] * factor * fin[...]).astype(BF)
    with jax.named_scope("drain"):
        for i, st in enumerate(streams):
            sent(others(st["sizes"][0] * lanes(i)), zs.at[i])
            sent(others(st["sizes"][1] * lanes(i)), ys.at[i])
        for family in range(4):
            sent(X.at[pl.ds(0, n_tp - 1)], xs.at[family])
        sent(Q.at[pl.ds(0, n_tp - 1)], xs.at[4])


def body(n_fs, n_tp, tokens, attn_gain, w_query, w_key, w_value, w_low, w_lift, decay_bias, head_gain,
         w_out, ffn_gain, w_gate, w_up, w_down, final_gain):
    rows, width = tokens.shape
    d_model = width * n_tp
    units = w_gate.shape[1]
    kq, ko, kd = w_query.shape[0], w_out.shape[0], w_down.shape[0]
    kd_pad = (kd + 127) // 128 * 128
    any_space = pl.BlockSpec(memory_space=pl.ANY)
    vmem = pl.BlockSpec(memory_space=pltpu.VMEM)

    def scratch(*shape, dtype=BF):
        return pltpu.VMEM(shape, dtype)

    def exchange():
        return [
            scratch(4, rows, width), scratch(4, rows, width), scratch(3, rows, width),
            scratch(2, rows, width), scratch(2, rows // 2, width), scratch(2, rows // 2, width, dtype=F32),
        ]

    half = n_fs // 2
    n_streams = 11
    ring = pltpu.SemaphoreType.DMA((n_streams, half))
    per_stream = pltpu.SemaphoreType.DMA((n_streams,))
    result = pl.pallas_call(
        functools.partial(kernel, n_fs, n_tp),
        out_shape=jax.ShapeDtypeStruct((rows, width), BF),
        in_specs=[any_space] * 15,
        out_specs=vmem,
        scratch_shapes=[
            scratch(w_low.shape[1], d_model),
            scratch(1, d_model, dtype=F32),
            scratch(*w_lift.shape),
            scratch(1, DK, dtype=F32),
            scratch(1, DV, dtype=F32),
            scratch(1, d_model, dtype=F32),
            scratch(1, width, dtype=F32),
            scratch(n_tp, rows, width),
            scratch(d_model, 2 * DK + DV),
            scratch(n_fs, ko, 128),
            scratch(n_fs, 2 * units, 128),
            scratch(n_fs, kd_pad, 128),
            scratch(rows, d_model),
            scratch(rows, 2 * DK + DV),
            scratch(rows, DK, dtype=F32),
            scratch(rows, DV),
            scratch(n_tp, rows, width),
            scratch(rows, kd_pad),
            scratch(rows, width, dtype=F32),
            scratch(n_tp, 8, 128, dtype=F32),
            scratch(DV, DK, dtype=F32),
            *exchange(),
            *exchange(),
            pltpu.SemaphoreType.DMA((15,)),
            per_stream, ring, per_stream, per_stream,
            pltpu.SemaphoreType.DMA((5,)),
            pltpu.SemaphoreType.DMA((61,)),
        ],
        compiler_params=pltpu.CompilerParams(
            collective_id=0, has_side_effects=True, vmem_limit_bytes=67043328
        ),
    )(
        tokens, w_query, w_key, w_value, w_out, w_gate.T, w_up.T, w_down,
        w_low.T, attn_gain.reshape(1, -1), w_lift, decay_bias.reshape(1, -1), head_gain.reshape(1, -1),
        ffn_gain.reshape(1, -1), final_gain.reshape(1, -1),
    )
    return result


def solution(mesh):
    n_fs, n_tp = mesh.shape["fs"], mesh.shape["tp"]
    if mesh.shape["grp"] % 2 or n_tp != 8:
        raise ValueError("unsupported mesh")
    return jax.shard_map(
        functools.partial(body, n_fs, n_tp),
        mesh=mesh,
        in_specs=(
            P(("grp", "fs"), "tp"),
            P(),
            P("fs", "tp"),
            P("fs", "tp"),
            P("fs", "tp"),
            P(),
            P(None, "tp"),
            P("tp"),
            P(),
            P("tp", "fs"),
            P(),
            P("fs", "tp"),
            P("fs", "tp"),
            P("tp", "fs"),
            P("tp"),
        ),
        out_specs=P(("grp", "fs"), "tp"),
        check_vma=False,
    )
```

```python
import functools

import jax
import jax.numpy as jnp
from jax import lax
from jax.experimental import pallas as pl
from jax.experimental.pallas import tpu as pltpu
from jax.sharding import PartitionSpec as P

DK = 128
DV = 256
BLOCK = 64
EPS = 1e-06
START, LATENCY, RATE = 2.3, 2.6, 46.6e3
BF = jnp.bfloat16
F32 = jnp.float32
MESH = pl.DeviceIdType.MESH
HIGHEST = lax.Precision.HIGHEST


def dot(a, b, dims=((1,), (0,)), precision=None):
    return lax.dot_general(
        a, b, (dims, ((), ())), precision=precision, preferred_element_type=F32
    )


def kernel(
    n_fs, n_tp,
    tok, wq, wk, wv, wo, wg, wu, wd, wl_in, ag_in, wlift_in, bias_in, hg_in, fg_in, fin_in,
    out,
    wl, ag, wlift, bias, hg, fg, fin,
    X, Gq, Go, Gg, Gd, N, QKV, C, M, F, H, SS, Q, state,
    PB1, D1, S1, B1, A1, T1, PB2, D2, S2, B2, A2, T2,
    lsem, zs, zr, ys, yr, xs, xr,
):
    rows, width = tok.shape
    d_model = width * n_tp
    half_rows = rows // 2
    half = n_fs // 2
    units = wg.shape[0]
    kq, ko, kd = wq.shape[0], wo.shape[0], wd.shape[0]

    grp, z, me = lax.axis_index("grp"), lax.axis_index("fs"), lax.axis_index("tp")
    parity = lax.rem(grp, 2)
    partner = {"grp": grp + 1 - 2 * parity}
    z_up, z_down = {"fs": lax.rem(z + 1, n_fs)}, {"fs": lax.rem(z + n_fs - 1, n_fs)}
    core = lax.rem(me, 2)

    def at_tp(offset):
        return lax.rem(me + offset + n_tp, n_tp)

    def other(slot):
        return slot + 1 - 2 * core

    r_slot, l_slot, o_slot = at_tp(2), at_tp(-2), at_tp(4)
    right, left, sib = {"tp": r_slot}, {"tp": l_slot}, {"tp": other(me)}

    def remote(src, dst, ssem, rsem, device):
        return pltpu.make_async_remote_copy(
            src_ref=src, dst_ref=dst, send_sem=ssem, recv_sem=rsem,
            device_id=device, device_id_type=MESH,
        )

    def send(src, dst, ssem, rsem, device):
        remote(src, dst, ssem, rsem, device).start()

    def arrived(ref, rsem):
        remote(ref, ref, xs.at[0], rsem, sib).wait_recv()

    def sent(ref, ssem):
        remote(ref, ref, ssem, xr.at[0], sib).wait_send()

    barrier = pltpu.get_barrier_semaphore()
    greeted = [z_up, z_down, partner] + [{"tp": at_tp(k)} for k in range(1, n_tp)]
    for device in greeted:
        pl.semaphore_signal(barrier, inc=1, device_id=device, device_id_type=MESH)
    zq = pl.multiple_of(z * kq, kq)
    local = [
        (tok, X.at[me]),
        (wq, Gq.at[pl.ds(zq, kq), pl.ds(0, DK)]),
        (wk, Gq.at[pl.ds(zq, kq), pl.ds(DK, DK)]),
        (wv, Gq.at[pl.ds(zq, kq), pl.ds(2 * DK, DV)]),
        (wo, Go.at[z]),
        (wg, Gg.at[z, pl.ds(0, units), :]),
        (wu, Gg.at[z, pl.ds(units, units), :]),
        (wd, Gd.at[z, pl.ds(0, kd), :]),
    ]
    local = [pltpu.make_async_copy(s, d, lsem.at[i]) for i, (s, d) in enumerate(local)]
    for copy in local:
        copy.start()

    small = [(wl_in, wl), (ag_in, ag), (wlift_in, wlift), (bias_in, bias), (hg_in, hg), (fg_in, fg), (fin_in, fin)]
    small = [pltpu.make_async_copy(s, d, lsem.at[8 + i]) for i, (s, d) in enumerate(small)]
    for copy in small:
        copy.start()

    if kd < Gd.shape[1]:
        Gd[:, kd:, :] = jnp.zeros((n_fs, Gd.shape[1] - kd, 128), BF)
        H[:, units:] = jnp.zeros((rows, H.shape[1] - units), BF)
    pl.semaphore_wait(barrier, len(greeted))

    def by_rows(view, base, total, edge):
        chunk, other_edge = total - edge, total - edge

        def part(shard, start, size):
            return view(shard, pl.multiple_of(base + start, 16), size)

        first = (chunk // 2 + 15) // 16 * 16
        return dict(
            ring=lambda s: part(s, parity * edge, chunk),
            mine=lambda s: part(s, parity * other_edge, edge),
            theirs=lambda s: part(s, (1 - parity) * other_edge, edge),
            sizes=(chunk, edge),
            halves=(
                lambda s: part(s, parity * edge, first),
                lambda s: part(s, parity * edge + first, chunk - first),
            ),
        )

    def view_q(shard, start, size):
        return Gq.at[pl.ds(pl.multiple_of(shard * kq + start, 16), size), :]

    def view_of(G):
        return lambda shard, start, size: G.at[shard, pl.ds(start, size), :]

    half_q, half_d, tail = kq // 2, kd // 2, units - 2 * 256
    streams = [
        by_rows(view_q, 0, half_q, 16),
        by_rows(view_q, half_q, half_q, 32),
        by_rows(view_of(Go), 0, ko, 96),
        by_rows(view_of(Gg), 0, 256, 112),
        by_rows(view_of(Gg), units, 256, 112),
        by_rows(view_of(Gg), 256, 256, 112),
        by_rows(view_of(Gg), units + 256, 256, 112),
        by_rows(view_of(Gg), 512, tail, tail // 32 * 16),
        by_rows(view_of(Gg), units + 512, tail, tail // 32 * 16),
        by_rows(view_of(Gd), 0, half_d, 0),
        by_rows(view_of(Gd), half_d, half_d, 0),
    ]
    QA, QB, OS, G0, U0, G1, U1, G2, U2, E0, E1 = range(11)

    def launch(i):
        ref = streams[i]["ring"](z)
        send(ref, ref, zs.at[i], zr.at[i, 0], z_up)
        send(ref, ref, zs.at[i], zr.at[i, 0], z_down)

    def event(i, s):
        st = streams[i]
        flows = ((lax.rem(z - s + n_fs, n_fs), z_up), (lax.rem(z + s, n_fs), z_down))
        arrived(some(1 if s == half else 2, st["sizes"][0] * lanes(i)), zr.at[i, s - 1])
        for way, (shard, device) in enumerate(flows):
            if s < half:
                ref = st["ring"](shard) if s + 1 < half else st["halves"][way](shard)
                send(ref, ref, zs.at[i], zr.at[i, s], device)
        for way, (shard, device) in enumerate(flows):
            if st["sizes"][1] and (s < half or way == 1):
                ref = st["mine"](shard)
                send(ref, ref, ys.at[i], yr.at[i], partner)

    def some(shards, size):
        return Gg.at[pl.ds(0, shards), pl.ds(0, size), :]

    def others(size):
        return some(n_fs - 1, size)

    def lanes(i):
        return 4 if i in (QA, QB) else 1

    def imported(*which):
        for i in which:
            if streams[i]["sizes"][1]:
                arrived(others(streams[i]["sizes"][1] * lanes(i)), yr.at[i])

    queue = []

    left_at, clock, link = {}, [START], [START]

    def due(until=None):
        until = clock[0] if until is None else until
        while queue:
            i, s = queue[0]
            arrival = left_at[i, s - 1] + LATENCY if s else clock[0]
            if arrival > until:
                break
            queue.pop(0)
            with jax.named_scope("ev%d_%d" % (i, s)):
                if s == 0:
                    launch(i)
                else:
                    event(i, s)
            clock[0] = max(clock[0], arrival) + (0.1 if s else 0.0)
            if s < half:
                weight = streams[i]["sizes"][0] * lanes(i) * 256 / RATE
                link[0] = max(link[0], clock[0]) + weight * (0.5 if s == half - 1 else 1)
                left_at[i, s] = link[0]
        clock[0] = max(clock[0], min(until, 1000.0))

    def due_to(*item):
        while item in queue:
            i, s = queue[0]
            due(left_at[i, s - 1] + LATENCY if s else clock[0])

    def work(us):
        clock[0] += us
        due()

    top, low = pl.ds(0, half_rows), pl.ds(half_rows, half_rows)

    def gather_stages(buf, base, family):
        def go(k, slot, part, device):
            ref = buf.at[slot] if part is None else buf.at[slot, part, :]
            send(ref, ref, xs.at[family], xr.at[base + k], device)

        def got(k, slot, part):
            ref = buf.at[slot] if part is None else buf.at[slot, part, :]
            arrived(ref, xr.at[base + k])

        def s0():
            go(0, me, top, right)
            go(2, me, low, left)
            go(1, me, low, right)
            go(3, me, top, left)
            go(4, me, None, sib)

        def s1():
            got(0, l_slot, top)
            go(5, l_slot, top, right)
            go(6, l_slot, top, sib)
            got(2, r_slot, low)
            go(7, r_slot, low, left)
            go(8, r_slot, low, sib)

        def s2():
            got(1, l_slot, low)
            go(9, l_slot, low, sib)
            got(3, r_slot, top)
            go(10, r_slot, top, sib)

        def s3():
            got(5, o_slot, top)
            go(11, o_slot, top, sib)
            got(7, o_slot, low)
            go(12, o_slot, low, sib)

        def s4():
            got(4, other(me), None)
            got(6, other(l_slot), top)
            got(8, other(r_slot), low)
            got(9, other(l_slot), low)
            got(10, other(r_slot), top)
            got(11, other(o_slot), top)
            got(12, other(o_slot), low)

        return s0, s1, s2, s3, s4

    def scatter_stages(left_ref, G, PB, D, S, B, A, T, SS, base, family):
        def go(k, src, dst, device):
            send(src, dst, xs.at[family], xr.at[base + k], device)

        def got(k, dst):
            arrived(dst, xr.at[base + k])

        def product(slot, part):
            weight = jnp.concatenate([G[2 * slot], G[2 * slot + 1]], axis=1)
            return dot(left_ref[part, :], weight)

        def quarter(q):
            return pl.ds(q * (half_rows // 2), half_rows // 2)

        def s0(k, late=None):
            slot = other((o_slot, r_slot, l_slot, me)[k])

            def body():
                for part in (top, low):
                    PB[k, part, :] = product(slot, part).astype(BF)
                go(k, PB.at[k], D.at[k], sib)

            if late is None:
                body()
            else:
                last = lax.div(lax.rem(z + half, n_fs), 2)
                pl.when((slot == last) if late else (slot != last))(body)

        def s1(k):
            slot = (o_slot, r_slot, l_slot, me)[k]
            parts = [product(slot, part) for part in (top, low)]
            got(k, D.at[k])
            parts = [p + D[k, part, :].astype(F32) for p, part in zip(parts, (top, low))]
            if k == 0:
                for way in range(2):
                    S[0, (top, low)[way], :] = parts[way].astype(BF)
                for h in range(2):
                    for way in range(2):
                        src = S.at[0, quarter(2 * way + h), :]
                        go((4, 10, 5, 11)[2 * way + h], src, A.at[way, quarter(h), :], (right, left)[way])
            elif k == 1:
                S[1, low, :] = parts[1].astype(BF)
                go(6, S.at[1, low, :], B.at[0, low, :], right)
                T[0] = parts[0]
            elif k == 2:
                S[2, top, :] = parts[0].astype(BF)
                go(7, S.at[2, top, :], B.at[1, top, :], left)
                T[1] = parts[1]
            else:
                SS[top, :] = parts[0]
                SS[low, :] = parts[1]

        def s2(h):
            for way in range(2):
                q = quarter(2 * way + h)
                got((4, 10, 5, 11)[2 * way + h], A.at[way, quarter(h), :])
                S[1 + way, q, :] = (T[way, quarter(h), :] + A[way, quarter(h), :].astype(F32)).astype(BF)
                go((8, 12, 9, 13)[2 * way + h], S.at[1 + way, q, :], B.at[way, q, :], (right, left)[way])

        def s3():
            got(6, B.at[0, low, :])
            got(7, B.at[1, top, :])
            for k, way, q in ((8, 0, 0), (9, 1, 2), (12, 0, 1), (13, 1, 3)):
                got(k, B.at[way, quarter(q), :])

        def own(r):
            return SS[r, :] + B[0, r, :].astype(F32) + B[1, r, :].astype(F32)

        return s0, s1, s2, s3, own

    def normalize(buf, gain, part):
        step = 32

        @pl.loop(part * (rows // step // 4), (part + 1) * (rows // step // 4))
        def _(t):
            r = pl.ds(pl.multiple_of(t * step, step), step)
            blocks = [buf[j, r, :].astype(F32) for j in range(n_tp)]
            squares = blocks[0] * blocks[0]
            for b in blocks[1:]:
                squares = squares + b * b
            factor = lax.rsqrt(jnp.sum(squares, axis=1, keepdims=True) * (1.0 / d_model) + EPS)
            for j, b in enumerate(blocks):
                cols = pl.ds(j * width, width)
                N[r, cols] = (b * factor * gain[:, cols]).astype(BF)

    ti = lax.broadcasted_iota(jnp.int32, (BLOCK, BLOCK), 0)
    si = lax.broadcasted_iota(jnp.int32, (BLOCK, BLOCK), 1)

    def decay(part):
        tril = jnp.where(ti >= si, 1.0, 0.0).astype(BF)
        step = 2 * BLOCK

        @pl.loop(part * (rows // step // 4), (part + 1) * (rows // step // 4))
        def _(t):
            r = pl.ds(pl.multiple_of(t * step, step), step)
            rank = dot(N[r, :], wl[...], ((1,), (1,))).astype(BF)
            v = dot(rank, wlift[...]) + bias[...]
            log_decay = (jnp.minimum(v, 0.0) - jnp.log1p(jnp.exp(-jnp.abs(v)))) * (1.0 / 16.0)
            for k in range(2):
                part = log_decay[k * BLOCK : (k + 1) * BLOCK]
                hi = part.astype(BF)
                lo = (part - hi.astype(F32)).astype(BF)
                r2 = pl.ds(pl.multiple_of(t * step + k * BLOCK, BLOCK), BLOCK)
                C[r2, :] = dot(tril, hi) + dot(tril, lo)

    def project(t):
        step = rows // 4
        r = pl.ds(t * step, step)
        QKV[r, :] = dot(N[r, :], Gq[...]).astype(BF)

    def attend(t):
        r = pl.ds(t * BLOCK, BLOCK)
        c = C[r, :]
        last = C[pl.ds((t + 1) * BLOCK - 1, 1), :]
        q = QKV[r, pl.ds(0, DK)].astype(F32) * DK ** (-0.5)
        k = QKV[r, pl.ds(DK, DK)].astype(F32)
        v = QKV[r, pl.ds(2 * DK, DV)]
        q_dec = (q * jnp.exp(c)).astype(BF)
        k_dec = (k * jnp.exp(-c)).astype(BF)
        k_end = (k * jnp.exp(last - c)).astype(BF)
        scores = jnp.where(ti >= si, dot(q_dec, k_dec, ((1,), (1,))), 0.0).astype(BF)
        o = dot(scores, v)
        if t > 0:
            o = o + dot(q_dec, state[...].astype(BF), ((1,), (1,)))
        added = dot(v, k_end, ((0,), (0,)))
        state[...] = state[...] * jnp.exp(last) + added if t > 0 else added
        factor = lax.rsqrt(jnp.mean(o * o, axis=1, keepdims=True) + EPS)
        M[r, :] = (o * factor * hg[...]).astype(BF)

    def feed(t, at, size):
        step = rows // 2
        r = pl.ds(t * step, step)

        def product(start):
            weight = jnp.concatenate([Gg[j, pl.ds(start, size), :] for j in range(n_fs)], axis=1)
            return dot(N[r, :], weight, ((1,), (1,)))

        gate, up = product(at), product(units + at)
        H[r, pl.ds(at, size)] = (gate / (1.0 + jnp.exp(-gate)) * up).astype(BF)

    plan = (((QA, QB, OS, G0), 0), ((U0, G1, U1), 6), ((G2, U2), 7), ((E0, E1), 8))
    for r in range(half + 9):
        for group, start in plan:
            if 0 <= r - start <= half:
                queue += [(i, r - start) for i in group]

    def gather(buf, base, family):
        g0, g1, g2, g3, g4 = gather_stages(buf, base, family)
        g0()
        begun = clock[0]
        for stage, ready in ((g1, 5.1), (g2, 7.8), (g3, 10.3), (g4, 11.1)):
            due(begun + ready - 0.2)
            stage()
            work(0.1)

    def scatter(stages, early=False):
        s0, s1, s2, s3, own = stages
        if early:
            for k in range(4):
                s0(k, late=False)
            due(10000.0)
            for k in range(4):
                s0(k, late=True)
            s1(0)
        else:
            for k in range(3):
                s0(k)
                work(0.25)
            s1(0)
            s0(3)
            work(0.6)
        begun = clock[0] - 0.3
        for k in range(1, 4):
            s1(k)
            work(0.27)
        due(begun + 4.2)
        s2(0)
        work(0.1)
        due(begun + 5.4)
        s2(1)
        work(0.1)
        due(begun + 10.0)
        s3()
        return own

    local[0].wait()
    for copy in local[1:]:
        copy.wait()
    due()
    gather(X, 0, 0)
    for copy in small:
        copy.wait()
    for t in range(4):
        normalize(X, ag, t)
        work(0.55)
    for t in range(4):
        decay(t)
        work(0.6)
    due_to(QB, half)
    due(clock[0] + 7.0)
    imported(QA, QB)
    for t in range(4):
        project(t)
        work(0.37)
    for t in range(rows // BLOCK):
        attend(t)
        work(0.2)
    imported(OS)
    own = scatter(scatter_stages(M, Go, PB1, D1, S1, B1, A1, T1, SS, 13, 1))

    @pl.loop(0, rows // 64)
    def _(t):
        r = pl.ds(pl.multiple_of(t * 64, 64), 64)
        F[me, r, :] = (X[me, r, :].astype(F32) + own(r)).astype(BF)

    work(0.3)
    gather(F, 27, 2)
    for t in range(4):
        normalize(F, fg, t)
        work(0.55)
    due_to(E1, half - 2)
    imported(G0, U0, G1, U1)
    feed(0, 0, 256)
    feed(0, 256, 256)
    feed(1, 0, 256)
    clock[0] += 2.3
    due_to(E1, half - 1)
    feed(1, 256, 256)
    imported(G2, U2)
    for t in range(2):
        feed(t, 512, units - 512)
    own = scatter(scatter_stages(H, Gd, PB2, D2, S2, B2, A2, T2, SS, 40, 3), early=True)

    ones = jnp.ones((8, width), BF)
    row = lax.broadcasted_iota(jnp.int32, (8, 128), 0)

    def in_two(v):
        hi = v.astype(BF)
        return hi, (v - hi.astype(F32)).astype(BF)

    with jax.named_scope("second"):
        packed = jnp.zeros((8, 128), F32)
        for b in range(rows // 128):
            part = pl.ds(b * 128, 128)
            second = F[me, part, :].astype(F32) + own(part)
            SS[part, :] = second
            sums = sum(dot(ones, v, ((1,), (1,))) for v in in_two(second * second))
            packed = jnp.where(row == b, sums, packed)
        Q[me] = packed
    with jax.named_scope("squares"):
        for k in (4, 5, 3, 2, 6, 7, 1):
            send(Q.at[me], Q.at[me], xs.at[4], xr.at[53 + k], {"tp": at_tp(k)})
        for k in range(1, n_tp):
            arrived(Q.at[at_tp(-k)], xr.at[53 + k])
    with jax.named_scope("close"):
        squares = Q[0]
        for j in range(1, n_tp):
            squares = squares + Q[j]
        factors = lax.rsqrt(squares * (1.0 / d_model) + EPS)
        for b in range(rows // 128):
            part = pl.ds(b * 128, 128)
            factor = sum(
                dot(v, ones, ((0,), (0,))) for v in in_two(jnp.where(row == b, factors, 0.0))
            )
            out[part, :] = (SS[part, :] * factor * fin[...]).astype(BF)
    with jax.named_scope("drain"):
        for i, st in enumerate(streams):
            sent(others(st["sizes"][0] * lanes(i)), zs.at[i])
            if st["sizes"][1]:
                sent(others(st["sizes"][1] * lanes(i)), ys.at[i])
        for family in range(4):
            sent(X.at[pl.ds(0, n_tp - 1)], xs.at[family])
        sent(Q.at[pl.ds(0, n_tp - 1)], xs.at[4])


def body(n_fs, n_tp, tokens, attn_gain, w_query, w_key, w_value, w_low, w_lift, decay_bias, head_gain,
         w_out, ffn_gain, w_gate, w_up, w_down, final_gain):
    rows, width = tokens.shape
    d_model = width * n_tp
    units = w_gate.shape[1]
    kq, ko, kd = w_query.shape[0], w_out.shape[0], w_down.shape[0]
    kd_pad = (kd + 127) // 128 * 128
    any_space = pl.BlockSpec(memory_space=pl.ANY)
    vmem = pl.BlockSpec(memory_space=pltpu.VMEM)

    def scratch(*shape, dtype=BF):
        return pltpu.VMEM(shape, dtype)

    def exchange():
        return [
            scratch(4, rows, width), scratch(4, rows, width), scratch(3, rows, width),
            scratch(2, rows, width), scratch(2, rows // 2, width), scratch(2, rows // 2, width, dtype=F32),
        ]

    half = n_fs // 2
    n_streams = 11
    ring = pltpu.SemaphoreType.DMA((n_streams, half))
    per_stream = pltpu.SemaphoreType.DMA((n_streams,))
    result = pl.pallas_call(
        functools.partial(kernel, n_fs, n_tp),
        out_shape=jax.ShapeDtypeStruct((rows, width), BF),
        in_specs=[any_space] * 15,
        out_specs=vmem,
        scratch_shapes=[
            scratch(w_low.shape[1], d_model),
            scratch(1, d_model, dtype=F32),
            scratch(*w_lift.shape),
            scratch(1, DK, dtype=F32),
            scratch(1, DV, dtype=F32),
            scratch(1, d_model, dtype=F32),
            scratch(1, width, dtype=F32),
            scratch(n_tp, rows, width),
            scratch(d_model, 2 * DK + DV),
            scratch(n_fs, ko, 128),
            scratch(n_fs, 2 * units, 128),
            scratch(n_fs, kd_pad, 128),
            scratch(rows, d_model),
            scratch(rows, 2 * DK + DV),
            scratch(rows, DK, dtype=F32),
            scratch(rows, DV),
            scratch(n_tp, rows, width),
            scratch(rows, kd_pad),
            scratch(rows, width, dtype=F32),
            scratch(n_tp, 8, 128, dtype=F32),
            scratch(DV, DK, dtype=F32),
            *exchange(),
            *exchange(),
            pltpu.SemaphoreType.DMA((15,)),
            per_stream, ring, per_stream, per_stream,
            pltpu.SemaphoreType.DMA((5,)),
            pltpu.SemaphoreType.DMA((61,)),
        ],
        compiler_params=pltpu.CompilerParams(
            collective_id=0, has_side_effects=True, vmem_limit_bytes=67043328
        ),
    )(
        tokens, w_query, w_key, w_value, w_out, w_gate.T, w_up.T, w_down,
        w_low.T, attn_gain.reshape(1, -1), w_lift, decay_bias.reshape(1, -1), head_gain.reshape(1, -1),
        ffn_gain.reshape(1, -1), final_gain.reshape(1, -1),
    )
    return result


def solution(mesh):
    n_fs, n_tp = mesh.shape["fs"], mesh.shape["tp"]
    if mesh.shape["grp"] % 2 or n_tp != 8:
        raise ValueError("unsupported mesh")
    return jax.shard_map(
        functools.partial(body, n_fs, n_tp),
        mesh=mesh,
        in_specs=(
            P(("grp", "fs"), "tp"),
            P(),
            P("fs", "tp"),
            P("fs", "tp"),
            P("fs", "tp"),
            P(),
            P(None, "tp"),
            P("tp"),
            P(),
            P("tp", "fs"),
            P(),
            P("fs", "tp"),
            P("fs", "tp"),
            P("tp", "fs"),
            P("tp"),
        ),
        out_specs=P(("grp", "fs"), "tp"),
        check_vma=False,
    )
```

```python
import functools

import jax
import jax.numpy as jnp
from jax import lax
from jax.experimental import pallas as pl
from jax.experimental.pallas import tpu as pltpu
from jax.sharding import PartitionSpec as P

DK = 128
DV = 256
BLOCK = 64
EPS = 1e-06
START, LATENCY, RATE = 2.3, 2.6, 46.6e3
BF = jnp.bfloat16
F32 = jnp.float32
MESH = pl.DeviceIdType.MESH
HIGHEST = lax.Precision.HIGHEST


def dot(a, b, dims=((1,), (0,)), precision=None):
    return lax.dot_general(
        a, b, (dims, ((), ())), precision=precision, preferred_element_type=F32
    )


def kernel(
    n_fs, n_tp,
    tok, wq, wk, wv, wo, wg, wu, wd, wl_in, ag_in, wlift_in, bias_in, hg_in, fg_in, fin_in,
    out,
    wl, ag, wlift, bias, hg, fg, fin,
    X, Gq, Go, Gg, Gd, N, QKV, C, M, F, H, SS, Q, state,
    PB1, D1, S1, B1, A1, T1, PB2, D2, S2, B2, A2, T2,
    lsem, zs, zr, ys, yr, xs, xr,
):
    rows, width = tok.shape
    d_model = width * n_tp
    half_rows = rows // 2
    half = n_fs // 2
    units = wg.shape[0]
    kq, ko, kd = wq.shape[0], wo.shape[0], wd.shape[0]

    grp, z, me = lax.axis_index("grp"), lax.axis_index("fs"), lax.axis_index("tp")
    parity = lax.rem(grp, 2)
    partner = {"grp": grp + 1 - 2 * parity}
    z_up, z_down = {"fs": lax.rem(z + 1, n_fs)}, {"fs": lax.rem(z + n_fs - 1, n_fs)}
    core = lax.rem(me, 2)

    def at_tp(offset):
        return lax.rem(me + offset + n_tp, n_tp)

    def other(slot):
        return slot + 1 - 2 * core

    r_slot, l_slot, o_slot = at_tp(2), at_tp(-2), at_tp(4)
    right, left, sib = {"tp": r_slot}, {"tp": l_slot}, {"tp": other(me)}

    def remote(src, dst, ssem, rsem, device):
        return pltpu.make_async_remote_copy(
            src_ref=src, dst_ref=dst, send_sem=ssem, recv_sem=rsem,
            device_id=device, device_id_type=MESH,
        )

    def send(src, dst, ssem, rsem, device):
        remote(src, dst, ssem, rsem, device).start()

    def arrived(ref, rsem):
        remote(ref, ref, xs.at[0], rsem, sib).wait_recv()

    def sent(ref, ssem):
        remote(ref, ref, ssem, xr.at[0], sib).wait_send()

    barrier = pltpu.get_barrier_semaphore()
    greeted = [z_up, z_down, partner] + [{"tp": at_tp(k)} for k in range(1, n_tp)]
    for device in greeted:
        pl.semaphore_signal(barrier, inc=1, device_id=device, device_id_type=MESH)
    zq = pl.multiple_of(z * kq, kq)
    local = [
        (tok, X.at[me]),
        (wq, Gq.at[pl.ds(zq, kq), pl.ds(0, DK)]),
        (wk, Gq.at[pl.ds(zq, kq), pl.ds(DK, DK)]),
        (wv, Gq.at[pl.ds(zq, kq), pl.ds(2 * DK, DV)]),
        (wo, Go.at[z]),
        (wg, Gg.at[z, pl.ds(0, units), :]),
        (wu, Gg.at[z, pl.ds(units, units), :]),
        (wd, Gd.at[z, pl.ds(0, kd), :]),
    ]
    local = [pltpu.make_async_copy(s, d, lsem.at[i]) for i, (s, d) in enumerate(local)]
    for copy in local:
        copy.start()

    small = [(wl_in, wl), (ag_in, ag), (wlift_in, wlift), (bias_in, bias), (hg_in, hg), (fg_in, fg), (fin_in, fin)]
    small = [pltpu.make_async_copy(s, d, lsem.at[8 + i]) for i, (s, d) in enumerate(small)]
    for copy in small:
        copy.start()

    if kd < Gd.shape[1]:
        Gd[:, kd:, :] = jnp.zeros((n_fs, Gd.shape[1] - kd, 128), BF)
        H[:, units:] = jnp.zeros((rows, H.shape[1] - units), BF)
    pl.semaphore_wait(barrier, len(greeted))

    def by_rows(view, base, total, edge):
        chunk, other_edge = total - edge, total - edge

        def part(shard, start, size):
            return view(shard, pl.multiple_of(base + start, 16), size)

        first = (chunk // 2 + 15) // 16 * 16
        return dict(
            ring=lambda s: part(s, parity * edge, chunk),
            mine=lambda s: part(s, parity * other_edge, edge),
            theirs=lambda s: part(s, (1 - parity) * other_edge, edge),
            sizes=(chunk, edge),
            halves=(
                lambda s: part(s, parity * edge, first),
                lambda s: part(s, parity * edge + first, chunk - first),
            ),
        )

    def view_q(shard, start, size):
        return Gq.at[pl.ds(pl.multiple_of(shard * kq + start, 16), size), :]

    def view_of(G):
        return lambda shard, start, size: G.at[shard, pl.ds(start, size), :]

    half_q, half_d, tail = kq // 2, kd // 2, units - 2 * 256
    streams = [
        by_rows(view_q, 0, half_q, 16),
        by_rows(view_q, half_q, half_q, 32),
        by_rows(view_of(Go), 0, ko, 96),
        by_rows(view_of(Gg), 0, 256, 112),
        by_rows(view_of(Gg), units, 256, 112),
        by_rows(view_of(Gg), 256, 256, 112),
        by_rows(view_of(Gg), units + 256, 256, 112),
        by_rows(view_of(Gg), 512, tail, tail // 32 * 16),
        by_rows(view_of(Gg), units + 512, tail, tail // 32 * 16),
        by_rows(view_of(Gd), 0, half_d, 0),
        by_rows(view_of(Gd), half_d, half_d, 0),
    ]
    QA, QB, OS, G0, U0, G1, U1, G2, U2, E0, E1 = range(11)

    def launch(i):
        ref = streams[i]["ring"](z)
        send(ref, ref, zs.at[i], zr.at[i, 0], z_up)
        send(ref, ref, zs.at[i], zr.at[i, 0], z_down)

    def event(i, s):
        st = streams[i]
        flows = ((lax.rem(z - s + n_fs, n_fs), z_up), (lax.rem(z + s, n_fs), z_down))
        arrived(some(1 if s == half else 2, st["sizes"][0] * lanes(i)), zr.at[i, s - 1])
        for way, (shard, device) in enumerate(flows):
            if s < half:
                ref = st["ring"](shard) if s + 1 < half else st["halves"][way](shard)
                send(ref, ref, zs.at[i], zr.at[i, s], device)
        for way, (shard, device) in enumerate(flows):
            if st["sizes"][1] and (s < half or way == 1):
                ref = st["mine"](shard)
                send(ref, ref, ys.at[i], yr.at[i], partner)

    def some(shards, size):
        return Gg.at[pl.ds(0, shards), pl.ds(0, size), :]

    def others(size):
        return some(n_fs - 1, size)

    def lanes(i):
        return 4 if i in (QA, QB) else 1

    def imported(*which):
        for i in which:
            if streams[i]["sizes"][1]:
                arrived(others(streams[i]["sizes"][1] * lanes(i)), yr.at[i])

    queue = []

    left_at, clock, link = {}, [START], [START]

    def due(until=None):
        until = clock[0] if until is None else until
        while queue:
            i, s = queue[0]
            arrival = left_at[i, s - 1] + LATENCY if s else clock[0]
            if arrival > until:
                break
            queue.pop(0)
            with jax.named_scope("ev%d_%d" % (i, s)):
                if s == 0:
                    launch(i)
                else:
                    event(i, s)
            clock[0] = max(clock[0], arrival) + (0.1 if s else 0.0)
            if s < half:
                weight = streams[i]["sizes"][0] * lanes(i) * 256 / RATE
                link[0] = max(link[0], clock[0]) + weight * (0.5 if s == half - 1 else 1)
                left_at[i, s] = link[0]
        clock[0] = max(clock[0], min(until, 1000.0))

    def due_to(*item):
        while item in queue:
            i, s = queue[0]
            due(left_at[i, s - 1] + LATENCY if s else clock[0])

    def work(us):
        clock[0] += us
        due()

    top, low = pl.ds(0, half_rows), pl.ds(half_rows, half_rows)

    def gather_stages(buf, base, family):
        def go(k, slot, part, device):
            ref = buf.at[slot] if part is None else buf.at[slot, part, :]
            send(ref, ref, xs.at[family], xr.at[base + k], device)

        def got(k, slot, part):
            ref = buf.at[slot] if part is None else buf.at[slot, part, :]
            arrived(ref, xr.at[base + k])

        def s0():
            go(0, me, top, right)
            go(2, me, low, left)
            go(1, me, low, right)
            go(3, me, top, left)
            go(4, me, None, sib)

        def s1():
            got(0, l_slot, top)
            go(5, l_slot, top, right)
            go(4, l_slot, top, sib)
            got(2, r_slot, low)
            go(6, r_slot, low, left)
            go(4, r_slot, low, sib)

        def s2():
            got(1, l_slot, low)
            go(4, l_slot, low, sib)
            got(3, r_slot, top)
            go(4, r_slot, top, sib)

        def s3():
            got(5, o_slot, top)
            go(4, o_slot, top, sib)
            got(6, o_slot, low)
            go(4, o_slot, low, sib)

        def s4():
            arrived(buf.at[pl.ds(0, n_tp // 2)], xr.at[base + 4])

        return s0, s1, s2, s3, s4

    def scatter_stages(left_ref, G, PB, D, S, B, A, T, SS, base, family):
        def go(k, src, dst, device):
            send(src, dst, xs.at[family], xr.at[base + k], device)

        def got(k, dst):
            arrived(dst, xr.at[base + k])

        def product(slot, part):
            weight = jnp.concatenate([G[2 * slot], G[2 * slot + 1]], axis=1)
            return dot(left_ref[part, :], weight)

        def quarter(q):
            return pl.ds(q * (half_rows // 2), half_rows // 2)

        def s0(k, late=None):
            slot = other((o_slot, r_slot, l_slot, me)[k])

            def body():
                for part in (top, low):
                    PB[k, part, :] = product(slot, part).astype(BF)
                go(k, PB.at[k], D.at[k], sib)

            if late is None:
                body()
            else:
                last = lax.div(lax.rem(z + half, n_fs), 2)
                pl.when((slot == last) if late else (slot != last))(body)

        def s1(k):
            slot = (o_slot, r_slot, l_slot, me)[k]
            parts = [product(slot, part) for part in (top, low)]
            got(k, D.at[k])
            parts = [p + D[k, part, :].astype(F32) for p, part in zip(parts, (top, low))]
            if k == 0:
                for way in range(2):
                    S[0, (top, low)[way], :] = parts[way].astype(BF)
                for h in range(2):
                    for way in range(2):
                        src = S.at[0, quarter(2 * way + h), :]
                        go((4, 5, 6, 7)[2 * way + h], src, A.at[way, quarter(h), :], (right, left)[way])
            elif k == 1:
                S[1, low, :] = parts[1].astype(BF)
                go(8, S.at[1, low, :], B.at[0, low, :], right)
                T[0] = parts[0]
            elif k == 2:
                S[2, top, :] = parts[0].astype(BF)
                go(8, S.at[2, top, :], B.at[1, top, :], left)
                T[1] = parts[1]
            else:
                SS[top, :] = parts[0]
                SS[low, :] = parts[1]

        def s2(h):
            for way in range(2):
                q = quarter(2 * way + h)
                got((4, 5, 6, 7)[2 * way + h], A.at[way, quarter(h), :])
                S[1 + way, q, :] = (T[way, quarter(h), :] + A[way, quarter(h), :].astype(F32)).astype(BF)
                go(8, S.at[1 + way, q, :], B.at[way, q, :], (right, left)[way])

        def s3():
            got(8, B)

        def own(r):
            return SS[r, :] + B[0, r, :].astype(F32) + B[1, r, :].astype(F32)

        return s0, s1, s2, s3, own

    def normalize(buf, gain, part):
        step = 32

        @pl.loop(part * (rows // step // 4), (part + 1) * (rows // step // 4))
        def _(t):
            r = pl.ds(pl.multiple_of(t * step, step), step)
            blocks = [buf[j, r, :].astype(F32) for j in range(n_tp)]
            squares = blocks[0] * blocks[0]
            for b in blocks[1:]:
                squares = squares + b * b
            factor = lax.rsqrt(jnp.sum(squares, axis=1, keepdims=True) * (1.0 / d_model) + EPS)
            for j, b in enumerate(blocks):
                cols = pl.ds(j * width, width)
                N[r, cols] = (b * factor * gain[:, cols]).astype(BF)

    ti = lax.broadcasted_iota(jnp.int32, (BLOCK, BLOCK), 0)
    si = lax.broadcasted_iota(jnp.int32, (BLOCK, BLOCK), 1)

    def decay(part):
        tril = jnp.where(ti >= si, 1.0, 0.0).astype(BF)
        step = 2 * BLOCK

        @pl.loop(part * (rows // step // 4), (part + 1) * (rows // step // 4))
        def _(t):
            r = pl.ds(pl.multiple_of(t * step, step), step)
            rank = dot(N[r, :], wl[...], ((1,), (1,))).astype(BF)
            v = dot(rank, wlift[...]) + bias[...]
            log_decay = (jnp.minimum(v, 0.0) - jnp.log1p(jnp.exp(-jnp.abs(v)))) * (1.0 / 16.0)
            for k in range(2):
                part = log_decay[k * BLOCK : (k + 1) * BLOCK]
                hi = part.astype(BF)
                lo = (part - hi.astype(F32)).astype(BF)
                r2 = pl.ds(pl.multiple_of(t * step + k * BLOCK, BLOCK), BLOCK)
                C[r2, :] = dot(tril, hi) + dot(tril, lo)

    def project(t):
        step = rows // 4
        r = pl.ds(t * step, step)
        QKV[r, :] = dot(N[r, :], Gq[...]).astype(BF)

    def attend(t):
        r = pl.ds(t * BLOCK, BLOCK)
        c = C[r, :]
        last = C[pl.ds((t + 1) * BLOCK - 1, 1), :]
        q = QKV[r, pl.ds(0, DK)].astype(F32) * DK ** (-0.5)
        k = QKV[r, pl.ds(DK, DK)].astype(F32)
        v = QKV[r, pl.ds(2 * DK, DV)]
        q_dec = (q * jnp.exp(c)).astype(BF)
        k_dec = (k * jnp.exp(-c)).astype(BF)
        k_end = (k * jnp.exp(last - c)).astype(BF)
        scores = jnp.where(ti >= si, dot(q_dec, k_dec, ((1,), (1,))), 0.0).astype(BF)
        o = dot(scores, v)
        if t > 0:
            o = o + dot(q_dec, state[...].astype(BF), ((1,), (1,)))
        added = dot(v, k_end, ((0,), (0,)))
        state[...] = state[...] * jnp.exp(last) + added if t > 0 else added
        factor = lax.rsqrt(jnp.mean(o * o, axis=1, keepdims=True) + EPS)
        M[r, :] = (o * factor * hg[...]).astype(BF)

    def feed(t, at, size):
        step = rows // 2
        r = pl.ds(t * step, step)

        def product(start):
            weight = jnp.concatenate([Gg[j, pl.ds(start, size), :] for j in range(n_fs)], axis=1)
            return dot(N[r, :], weight, ((1,), (1,)))

        gate, up = product(at), product(units + at)
        H[r, pl.ds(at, size)] = (gate / (1.0 + jnp.exp(-gate)) * up).astype(BF)

    plan = (((QA, QB, OS, G0), 0), ((U0, G1, U1), 6), ((G2, U2), 7), ((E0, E1), 8))
    for r in range(half + 9):
        for group, start in plan:
            if 0 <= r - start <= half:
                queue += [(i, r - start) for i in group]

    def gather(buf, base, family):
        g0, g1, g2, g3, g4 = gather_stages(buf, base, family)
        g0()
        begun = clock[0]
        for stage, ready in ((g1, 5.1), (g2, 7.8), (g3, 10.3), (g4, 11.1)):
            due(begun + ready - 0.2)
            stage()
            work(0.1)

    def scatter(stages, early=False):
        s0, s1, s2, s3, own = stages
        if early:
            for k in range(4):
                s0(k, late=False)
            due(10000.0)
            for k in range(4):
                s0(k, late=True)
            s1(0)
        else:
            for k in range(3):
                s0(k)
                work(0.25)
            s1(0)
            s0(3)
            work(0.6)
        begun = clock[0] - 0.3
        for k in range(1, 4):
            s1(k)
            work(0.27)
        due(begun + 4.2)
        s2(0)
        work(0.1)
        due(begun + 5.4)
        s2(1)
        work(0.1)
        due(begun + 10.0)
        s3()
        return own

    local[0].wait()
    for copy in local[1:]:
        copy.wait()
    due()
    gather(X, 0, 0)
    for copy in small:
        copy.wait()
    for t in range(4):
        normalize(X, ag, t)
        work(0.55)
    for t in range(4):
        decay(t)
        work(0.6)
    due_to(QB, half)
    due(clock[0] + 7.0)
    imported(QA, QB)
    for t in range(4):
        project(t)
        work(0.37)
    for t in range(rows // BLOCK):
        attend(t)
        work(0.2)
    imported(OS)
    own = scatter(scatter_stages(M, Go, PB1, D1, S1, B1, A1, T1, SS, 7, 1))

    @pl.loop(0, rows // 64)
    def _(t):
        r = pl.ds(pl.multiple_of(t * 64, 64), 64)
        F[me, r, :] = (X[me, r, :].astype(F32) + own(r)).astype(BF)

    work(0.3)
    gather(F, 16, 2)
    for t in range(4):
        normalize(F, fg, t)
        work(0.55)
    due_to(E1, half - 2)
    imported(G0, U0, G1, U1)
    feed(0, 0, 256)
    feed(0, 256, 256)
    feed(1, 0, 256)
    clock[0] += 2.3
    due_to(E1, half - 1)
    feed(1, 256, 256)
    imported(G2, U2)
    for t in range(2):
        feed(t, 512, units - 512)
    own = scatter(scatter_stages(H, Gd, PB2, D2, S2, B2, A2, T2, SS, 23, 3), early=True)

    ones = jnp.ones((8, width), BF)
    row = lax.broadcasted_iota(jnp.int32, (8, 128), 0)

    def in_two(v):
        hi = v.astype(BF)
        return hi, (v - hi.astype(F32)).astype(BF)

    with jax.named_scope("second"):
        packed = jnp.zeros((8, 128), F32)
        for b in range(rows // 128):
            part = pl.ds(b * 128, 128)
            second = F[me, part, :].astype(F32) + own(part)
            SS[part, :] = second
            sums = sum(dot(ones, v, ((1,), (1,))) for v in in_two(second * second))
            packed = jnp.where(row == b, sums, packed)
        Q[me] = packed
    with jax.named_scope("squares"):
        for k in (4, 5, 3, 2, 6, 7, 1):
            send(Q.at[me], Q.at[me], xs.at[4], xr.at[32], {"tp": at_tp(k)})
        arrived(Q.at[pl.ds(0, n_tp - 1)], xr.at[32])
    with jax.named_scope("close"):
        squares = Q[0]
        for j in range(1, n_tp):
            squares = squares + Q[j]
        factors = lax.rsqrt(squares * (1.0 / d_model) + EPS)
        for b in range(rows // 128):
            part = pl.ds(b * 128, 128)
            factor = sum(
                dot(v, ones, ((0,), (0,))) for v in in_two(jnp.where(row == b, factors, 0.0))
            )
            out[part, :] = (SS[part, :] * factor * fin[...]).astype(BF)
    with jax.named_scope("drain"):
        for i, st in enumerate(streams):
            sent(others(st["sizes"][0] * lanes(i)), zs.at[i])
            if st["sizes"][1]:
                sent(others(st["sizes"][1] * lanes(i)), ys.at[i])
        for family in range(4):
            sent(X.at[pl.ds(0, n_tp - 1)], xs.at[family])
        sent(Q.at[pl.ds(0, n_tp - 1)], xs.at[4])


def body(n_fs, n_tp, tokens, attn_gain, w_query, w_key, w_value, w_low, w_lift, decay_bias, head_gain,
         w_out, ffn_gain, w_gate, w_up, w_down, final_gain):
    rows, width = tokens.shape
    d_model = width * n_tp
    units = w_gate.shape[1]
    kq, ko, kd = w_query.shape[0], w_out.shape[0], w_down.shape[0]
    kd_pad = (kd + 127) // 128 * 128
    any_space = pl.BlockSpec(memory_space=pl.ANY)
    vmem = pl.BlockSpec(memory_space=pltpu.VMEM)

    def scratch(*shape, dtype=BF):
        return pltpu.VMEM(shape, dtype)

    def exchange():
        return [
            scratch(4, rows, width), scratch(4, rows, width), scratch(3, rows, width),
            scratch(2, rows, width), scratch(2, rows // 2, width), scratch(2, rows // 2, width, dtype=F32),
        ]

    half = n_fs // 2
    n_streams = 11
    ring = pltpu.SemaphoreType.DMA((n_streams, half))
    per_stream = pltpu.SemaphoreType.DMA((n_streams,))
    result = pl.pallas_call(
        functools.partial(kernel, n_fs, n_tp),
        out_shape=jax.ShapeDtypeStruct((rows, width), BF),
        in_specs=[any_space] * 15,
        out_specs=vmem,
        scratch_shapes=[
            scratch(w_low.shape[1], d_model),
            scratch(1, d_model, dtype=F32),
            scratch(*w_lift.shape),
            scratch(1, DK, dtype=F32),
            scratch(1, DV, dtype=F32),
            scratch(1, d_model, dtype=F32),
            scratch(1, width, dtype=F32),
            scratch(n_tp, rows, width),
            scratch(d_model, 2 * DK + DV),
            scratch(n_fs, ko, 128),
            scratch(n_fs, 2 * units, 128),
            scratch(n_fs, kd_pad, 128),
            scratch(rows, d_model),
            scratch(rows, 2 * DK + DV),
            scratch(rows, DK, dtype=F32),
            scratch(rows, DV),
            scratch(n_tp, rows, width),
            scratch(rows, kd_pad),
            scratch(rows, width, dtype=F32),
            scratch(n_tp, 8, 128, dtype=F32),
            scratch(DV, DK, dtype=F32),
            *exchange(),
            *exchange(),
            pltpu.SemaphoreType.DMA((15,)),
            per_stream, ring, per_stream, per_stream,
            pltpu.SemaphoreType.DMA((5,)),
            pltpu.SemaphoreType.DMA((33,)),
        ],
        compiler_params=pltpu.CompilerParams(
            collective_id=0, has_side_effects=True, vmem_limit_bytes=67043328
        ),
    )(
        tokens, w_query, w_key, w_value, w_out, w_gate.T, w_up.T, w_down,
        w_low.T, attn_gain.reshape(1, -1), w_lift, decay_bias.reshape(1, -1), head_gain.reshape(1, -1),
        ffn_gain.reshape(1, -1), final_gain.reshape(1, -1),
    )
    return result


def solution(mesh):
    n_fs, n_tp = mesh.shape["fs"], mesh.shape["tp"]
    if mesh.shape["grp"] % 2 or n_tp != 8:
        raise ValueError("unsupported mesh")
    return jax.shard_map(
        functools.partial(body, n_fs, n_tp),
        mesh=mesh,
        in_specs=(
            P(("grp", "fs"), "tp"),
            P(),
            P("fs", "tp"),
            P("fs", "tp"),
            P("fs", "tp"),
            P(),
            P(None, "tp"),
            P("tp"),
            P(),
            P("tp", "fs"),
            P(),
            P("fs", "tp"),
            P("fs", "tp"),
            P("tp", "fs"),
            P("tp"),
        ),
        out_specs=P(("grp", "fs"), "tp"),
        check_vma=False,
    )
```
